256 devices in a mesh: ep: 128 (over z, y, x), tp: 2 (over core).
Axes of the slice: x: 4, y: 4, z: 8, core: 2. Of those that a mesh axis runs over, the one named last changes fastest.
Arguments:
- tokens: bfloat16 [2048, 2048], P('ep'), may hold values from -6 to 6
- lengths: int32 [2048], P('ep'), may hold values from 1 to 1024, as said below
- attn_gain: float32 [2048], replicated, may hold values from 0.1 to 1.9
- w_query: bfloat16 [2048, 1024], P(None, 'tp'), may hold values from -0.125 to 0.125
- w_key: bfloat16 [2048, 128], P(None, 'tp'), may hold values from -0.125 to 0.125
- w_value: bfloat16 [2048, 128], P(None, 'tp'), may hold values from -0.125 to 0.125
- head_bias: float32 [16], P('tp'), may hold values from -7 to -2
- key_cache: bfloat16 [2048, 2, 64, 1024], P('ep', 'tp'), may hold values from -6 to 6
- value_cache: bfloat16 [2048, 2, 64, 1024], P('ep', 'tp'), may hold values from -6 to 6
- w_attn_out: bfloat16 [1024, 2048], P('tp'), may hold values from -0.1875 to 0.1875
- ffn_gain: float32 [2048], replicated, may hold values from 0.1 to 1.9
- w_router: bfloat16 [2048, 128], replicated, may hold values from -0.125 to 0.125
- routes: int32 [2048, 6], P('ep'), may hold values from 0 to 127, all different within a row; in each aligned block of 16 rows (0 to 15, 16 to 31, ...) at most 2 rows name the same one
- w_dense_gate: bfloat16 [2048, 512], P('ep', 'tp'), may hold values from -0.125 to 0.125
- w_dense_up: bfloat16 [2048, 512], P('ep', 'tp'), may hold values from -0.125 to 0.125
- w_dense_down: bfloat16 [512, 2048], P('tp', 'ep'), may hold values from -0.25 to 0.25
- dense_mix: float32 [2048], replicated, may hold values from -0.125 to 0.125
- w_expert_gate: bfloat16 [128, 2048, 512], P('ep', None, 'tp'), may hold values from -0.125 to 0.125
- w_expert_up: bfloat16 [128, 2048, 512], P('ep', None, 'tp'), may hold values from -0.125 to 0.125
- w_expert_down: bfloat16 [128, 512, 2048], P('ep', 'tp'), may hold values from -0.25 to 0.25
Outputs:
- layer_out: bfloat16 [2048, 2048], P('ep', 'tp')
- new_keys: bfloat16 [2048, 128], P('ep', 'tp')
- new_values: bfloat16 [2048, 128], P('ep', 'tp')
The draws below stay inside these ranges and needn't reach their ends.
Inputs may be any that keep to these rules, and one draw needn't show every extreme that they name: `lengths`: every sequence holds between 1 and 1024 cached positions; in every draw some sequence holds exactly 1024. `routes`: each token names 6 different experts. Among the rows of one device no expert is named by more than 2 rows.
All inputs are finite; a program needn't handle non-finite values.
Results may differ from the reference program's by a relative error of at most 0.014.
Values may be sent and summed in bfloat16 or wider, within the bound.
A program may use at most 64 MiB of HBM per device.

```python
import math
import jax
import jax.numpy as jnp
import numpy as np
from jax import lax

D = 2048
HEADS = 16
KV_HEADS = 2
HEAD = 64
EXPERT_WIDTH = 512
SHARED = 512
TOP_K = 6
SEQ_DEV = 16
CACHE = 1024
EXPERTS = 128
TOKENS = 2048
CAP = 2
N_EP = 128
N_TP = 2


def draw_lengths(key, part):
    key_caps = jax.random.fold_in(key, 11)
    key_rows = jax.random.fold_in(key, 12)
    key_full = jax.random.fold_in(key, 13)
    group_total = TOKENS // SEQ_DEV
    device_caps = jax.random.randint(key_caps, (group_total, 1), CACHE // 8, CACHE + 1)
    drawn = jax.random.randint(key_rows, (group_total, SEQ_DEV), 1, device_caps + 1).reshape(-1)
    full_at = jax.random.randint(key_full, (), 0, TOKENS)
    drawn = jnp.where(jnp.arange(TOKENS, dtype=jnp.int32) == full_at, CACHE, drawn)
    return drawn.astype(jnp.int32)


def levels(rng, shape, pieces, least, top_value):
    level, own = 1.0, jax.random.fold_in(rng, 6)
    for position, shards_of in pieces:
        steps = jnp.exp(jax.random.uniform(jax.random.fold_in(own, position), (shards_of,), jnp.float32, least / len(pieces), top_value / len(pieces)))
        level = level * jnp.repeat(steps, shape[position] // shards_of).reshape([-1 if axis == position else 1 for axis in range(len(shape))])
    return level


def shared_out(own_key, own, number, rows, number_of, top, limit, slope):
    order = jax.random.permutation(own_key, number_of)
    crowded, ordinary = shares(number_of, rows * top, limit, slope, True), shares(number_of, rows * top, limit, slope, False)
    places = jnp.arange(number_of)

    def named(sizes, rotation):
        used = int((sizes > 0).sum())
        fixed = max(1, used // 4)
        shifted = fixed + (places - fixed + rotation * (used - fixed)) % max(1, number_of - fixed)
        return jnp.zeros((number_of,), jnp.int32).at[order[jnp.where(places < fixed, places, shifted)]].set(jnp.asarray(sizes, jnp.int32))

    sizes = jnp.where(number % 4 == 0, named(crowded, number // 4), named(ordinary, number - number // 4 - 1))
    mixed = jax.random.permutation(jax.random.fold_in(own, 3), number_of)
    donor, taker = mixed[0:number_of // 2 * 2:2], mixed[1:number_of // 2 * 2:2]
    margin = jnp.minimum(sizes[donor] - 1, limit - sizes[taker]) // 2
    margin = jnp.where((donor == order[0]) | (taker == order[0]) | (sizes[taker] == 0), 0, jnp.maximum(margin, 0))
    shifted = jax.random.randint(jax.random.fold_in(own, 4), (number_of // 2,), 0, 1 << 20) % (margin + 1)
    sizes = sizes.at[donor].add(-shifted).at[taker].add(shifted)
    members = jnp.searchsorted(jnp.cumsum(sizes), jnp.arange(rows * top), side="right").astype(jnp.int32)
    listing = members.reshape(top, rows).T
    listing = listing[jax.random.permutation(jax.random.fold_in(own, 1), rows)]
    rotation = jax.random.randint(jax.random.fold_in(own, 2), (rows, 1), 0, top)
    return jnp.take_along_axis(listing, (jnp.arange(top)[None, :] + rotation) % top, axis=1)


def shares(number_of, total, most, skew, full):
    loads = [(1 << 20) // math.isqrt(standing ** skew) + 1 for standing in range(1, number_of + 1)]
    largest = most if full else min(most, max(-(-total // number_of), total * loads[0] // sum(loads)))
    least = 1 if total - largest >= number_of - 1 else 0
    given, rest = [largest] + [least] * (number_of - 1), total - largest - least * (number_of - 1)
    while rest > 0:
        free = [i for i in range(1, number_of) if given[i] < largest] or [i for i in range(1, number_of) if given[i] < most]
        mass, budget = sum([loads[i] for i in free]), rest
        for i in free:
            addition = min(most - given[i], max(1, budget * loads[i] // mass), rest)
            given[i] = given[i] + addition
            rest = rest - addition
    return np.array(given)


def gaussian(own_key, extent, spread, most, split=(), held_as=jnp.bfloat16):
    level = levels(own_key, extent, split, -0.22, 0.18) if split else 1.0
    entries = jax.random.normal(own_key, extent, jnp.float32) * spread * level
    return jnp.minimum(jnp.maximum(entries, -most), most).astype(held_as)


def setup_inputs(seed: int = 0) -> dict:
    streams_of = jax.random.split(jax.random.key(seed), 21)
    tokens = gaussian(streams_of[0], (TOKENS, D), 1.0, 6.0, ((0, 128),))
    lengths = draw_lengths(jax.random.fold_in(streams_of[20], 71), 0)
    attn_gain = jnp.clip(1.0 + 0.18 * jax.random.normal(streams_of[2], (D,), jnp.float32), 0.1, 1.9)
    w_query = gaussian(streams_of[3], (D, HEADS * HEAD), D ** -0.5, 0.125, ((1, 2),))
    w_key = gaussian(streams_of[4], (D, KV_HEADS * HEAD), D ** -0.5, 0.125, ((1, 2),))
    w_value = gaussian(streams_of[5], (D, KV_HEADS * HEAD), D ** -0.5, 0.125, ((1, 2),))
    head_bias = jnp.clip(-7.0 + 5.0 * jax.random.uniform(streams_of[6], (HEADS,), jnp.float32) ** levels(streams_of[6], (HEADS,), ((0, 2),), -0.2, 0.2), -7.0, -2.0)
    key_cache = gaussian(streams_of[7], (TOKENS, KV_HEADS, HEAD, CACHE), 1.0, 6.0, ((0, 128), (1, 2)))
    value_cache = gaussian(streams_of[8], (TOKENS, KV_HEADS, HEAD, CACHE), 1.0, 6.0, ((0, 128), (1, 2)))
    w_attn_out = gaussian(streams_of[9], (HEADS * HEAD, D), (HEADS * HEAD) ** -0.5, 0.1875, ((0, 2),))
    ffn_gain = jnp.clip(1.0 + 0.18 * jax.random.normal(streams_of[10], (D,), jnp.float32), 0.1, 1.9)
    w_router = gaussian(streams_of[11], (D, EXPERTS), D ** -0.5, 0.125)
    routes_keys = jax.random.split(jax.random.fold_in(streams_of[12], 1), TOKENS // SEQ_DEV)
    routes_turns = jax.random.permutation(jax.random.fold_in(streams_of[12], 3), TOKENS // SEQ_DEV)
    routes = jax.vmap(lambda own, number: shared_out(jax.random.fold_in(streams_of[12], 2), own, number, SEQ_DEV, EXPERTS, TOP_K, CAP, 2))(routes_keys, routes_turns).reshape((TOKENS, TOP_K))
    w_dense_gate = gaussian(streams_of[13], (D, SHARED), D ** -0.5, 0.125, ((0, 128), (1, 2)))
    w_dense_up = gaussian(streams_of[14], (D, SHARED), D ** -0.5, 0.125, ((0, 128), (1, 2)))
    w_dense_down = gaussian(streams_of[15], (SHARED, D), SHARED ** -0.5, 0.25, ((0, 2), (1, 128)))
    dense_mix = gaussian(streams_of[16], (D,), D ** -0.5, 0.125, (), jnp.float32)
    w_expert_gate = gaussian(streams_of[17], (EXPERTS, D, EXPERT_WIDTH), D ** -0.5, 0.125, ((0, 128), (2, 2)))
    w_expert_up = gaussian(streams_of[18], (EXPERTS, D, EXPERT_WIDTH), D ** -0.5, 0.125, ((0, 128), (2, 2)))
    w_expert_down = gaussian(streams_of[19], (EXPERTS, EXPERT_WIDTH, D), EXPERT_WIDTH ** -0.5, 0.25, ((0, 128), (1, 2)))
    return {"tokens": tokens, "lengths": lengths, "attn_gain": attn_gain, "w_query": w_query, "w_key": w_key, "w_value": w_value, "head_bias": head_bias, "key_cache": key_cache, "value_cache": value_cache, "w_attn_out": w_attn_out, "ffn_gain": ffn_gain, "w_router": w_router, "routes": routes, "w_dense_gate": w_dense_gate, "w_dense_up": w_dense_up, "w_dense_down": w_dense_down, "dense_mix": dense_mix, "w_expert_gate": w_expert_gate, "w_expert_up": w_expert_up, "w_expert_down": w_expert_down}


def rms_scale(values, gain):
    wide = values.astype(jnp.float32)
    return wide * lax.rsqrt(lax.optimization_barrier(jnp.mean(wide * wide, axis=-1, keepdims=True)) + 1e-06) * gain

def halves_sum(hidden, down, rows):
    split_hidden = hidden.reshape(rows, N_TP, -1).astype(jnp.float32)
    split_down = down.reshape(N_TP, -1, D).astype(jnp.float32)
    parts = jnp.einsum('rnf,nfd->nrd', split_hidden, split_down).astype(jnp.bfloat16)
    return lax.optimization_barrier(jnp.sum(parts.astype(jnp.float32), axis=0))

def reference(tokens, lengths, attn_gain, w_query, w_key, w_value, head_bias, key_cache, value_cache, w_attn_out, ffn_gain, w_router, routes, w_dense_gate, w_dense_up, w_dense_down, dense_mix, w_expert_gate, w_expert_up, w_expert_down):
    normed = rms_scale(tokens, attn_gain).astype(jnp.bfloat16)
    queries = jnp.dot(normed, w_query, preferred_element_type=jnp.float32).astype(jnp.bfloat16)
    new_keys = jnp.dot(normed, w_key, preferred_element_type=jnp.float32).astype(jnp.bfloat16)
    new_values = jnp.dot(normed, w_value, preferred_element_type=jnp.float32).astype(jnp.bfloat16)
    group_size = HEADS // KV_HEADS
    block_total = TOKENS // SEQ_DEV
    grouped = queries.reshape(block_total, SEQ_DEV, KV_HEADS, group_size, HEAD)
    key_blocks = key_cache.reshape(block_total, SEQ_DEV, KV_HEADS, HEAD, CACHE)
    value_blocks = value_cache.reshape(block_total, SEQ_DEV, KV_HEADS, HEAD, CACHE)
    length_blocks = lengths.reshape(block_total, SEQ_DEV)
    head_shift = head_bias.reshape(1, KV_HEADS, group_size, 1)

    def attend(inputs):
        block_queries, block_keys, block_values, block_lengths = inputs
        scores = jnp.einsum('skgd,skdc->skgc', block_queries.astype(jnp.float32), block_keys.astype(jnp.float32)) * HEAD ** (-0.5) + head_shift
        visible = (jnp.arange(CACHE, dtype=jnp.int32)[None, :] < block_lengths[:, None])[:, None, None, :]
        log_keep = jnp.where(visible, jax.nn.log_sigmoid(-scores), 0.0)
        log_after = lax.cumsum(log_keep, axis=3, reverse=True) - log_keep
        weights = jnp.where(visible, jnp.exp(jax.nn.log_sigmoid(scores) + log_after), 0.0).astype(jnp.bfloat16)
        mixed = jnp.einsum('skgc,skdc->skgd', weights.astype(jnp.float32), block_values.astype(jnp.float32))
        return mixed.reshape(SEQ_DEV, HEADS * HEAD).astype(jnp.bfloat16)
    heads_out = lax.map(attend, (grouped, key_blocks, value_blocks, length_blocks)).reshape(TOKENS, HEADS * HEAD)
    attn = halves_sum(heads_out, w_attn_out, TOKENS)
    residual = (tokens.astype(jnp.float32) + attn).astype(jnp.bfloat16)
    normed2 = rms_scale(residual, ffn_gain).astype(jnp.bfloat16)
    probs = jax.nn.sigmoid(jnp.dot(normed2, w_router, preferred_element_type=jnp.float32))
    hits = routes[:, :, None] == jnp.arange(EXPERTS, dtype=jnp.int32)[None, None, :]
    picked = lax.optimization_barrier(jnp.sum(jnp.where(hits, probs[:, None, :], 0.0), axis=-1))
    gates = picked / lax.optimization_barrier(jnp.sum(picked, axis=-1, keepdims=True)) * 2.5
    flat_routes = routes.reshape(-1)
    route_total = TOKENS * TOP_K
    bound = N_EP * CAP
    padded_inputs = jnp.concatenate([normed2, jnp.zeros((1, D), jnp.bfloat16)], axis=0)

    def expert_pass(inputs):
        expert_id, gate_w, up_w, down_w = inputs
        chosen = jnp.nonzero(flat_routes == expert_id, size=bound, fill_value=route_total)[0].astype(jnp.int32)
        rows_in = padded_inputs[chosen // TOP_K]
        gate_rows = jnp.dot(rows_in, gate_w, preferred_element_type=jnp.float32)
        up_rows = jnp.dot(rows_in, up_w, preferred_element_type=jnp.float32)
        hidden = (jax.nn.silu(gate_rows) * up_rows).astype(jnp.bfloat16)
        return (halves_sum(hidden, down_w, bound).astype(jnp.bfloat16), chosen)
    expert_rows, chosen_all = lax.map(expert_pass, (jnp.arange(EXPERTS, dtype=jnp.int32), w_expert_gate, w_expert_up, w_expert_down))
    route_rows = jnp.zeros((route_total + 1, D), jnp.bfloat16).at[chosen_all.reshape(-1)].set(expert_rows.reshape(-1, D))[:route_total]
    routed = lax.optimization_barrier(jnp.sum(gates[:, :, None] * route_rows.reshape(TOKENS, TOP_K, D).astype(jnp.float32), axis=1))
    dense_gate_rows = jnp.dot(normed2, w_dense_gate, preferred_element_type=jnp.float32)
    dense_up_rows = jnp.dot(normed2, w_dense_up, preferred_element_type=jnp.float32)
    dense_hidden = (jax.nn.silu(dense_gate_rows) * dense_up_rows).astype(jnp.bfloat16)
    dense = halves_sum(dense_hidden, w_dense_down, TOKENS)
    mix_gate = jax.nn.sigmoid(lax.optimization_barrier(jnp.sum(normed2.astype(jnp.float32) * dense_mix, axis=-1)))
    layer_out = (residual.astype(jnp.float32) + mix_gate[:, None] * dense + routed).astype(jnp.bfloat16)
    return (layer_out, new_keys, new_values)
```

```python
import jax
import jax.numpy as jnp
from jax import lax
from jax.experimental import pallas as pl
from jax.experimental.pallas import tpu as pltpu
from jax.sharding import Mesh
from jax.sharding import PartitionSpec as P

EP = ("z", "y", "x")
MESH = pl.DeviceIdType.MESH
NZ, NY, NX = 8, 4, 4
PLANE = NY * NX
ROWS, WIDTH, HALF = 16, 2048, 1024
F32, BF16 = jnp.float32, jnp.bfloat16
NT = (((1,), (1,)), ((), ()))
LOADS = 21


def dot(a, b):
    return jnp.dot(a, b, preferred_element_type=F32)


def dot_nt(a, b):
    return lax.dot_general(a, b, NT, preferred_element_type=F32)


def iota(shape, dim):
    return lax.broadcasted_iota(jnp.int32, shape, dim)


def bits(mask):
    return jnp.where(mask, 1.0, 0.0).astype(BF16)


def two_terms(x):
    high = x.astype(BF16)
    return high, (x - high.astype(F32)).astype(BF16)


def sigmoid(x):
    return 1.0 / (1.0 + jnp.exp(-x))


def rms_scale(values, gain):
    wide = values.astype(F32)
    return (wide * lax.rsqrt(jnp.mean(wide * wide, axis=-1, keepdims=True) + 1e-06) * gain).astype(BF16)


def kernel(
    tokens_h, lengths, attn_gain_h, wq_h, wk_h, wv_h, head_bias, keys_h, values_h, wo_h,
    ffn_gain_h, wr_h, routes_h, wdg_h, wdu_h, wdd_h, mix_h, weg_h, weu_h, wed_h,
    out, new_keys, new_values,
    tokens, attn_gain, wq, wk, wv, keys, values, wo, ffn_gain, wr, routes, wdg, wdu, wdd, mixw,
    weg, weu, wed,
    w3p, w3, hits, gm, part, peer_part, norm2, resid, tokf, xs, xin, eo_mine, eo_send, eo_peer,
    ys, yr, dn_mine, dn_send, dn_peer, ps, pr,
    load_sem, w3z_s, w3z_r, w3x_s, w3x_r, w3y_s, w3y_r, h_s, h_r, ap_s, ap_r, tz_s, tz_r, g_s, g_r,
    tf_s, tf_r, xs_s, xs_r, xf_s, xf_r, eo_s, eo_r, ys_s, ys_r, dn_s, dn_r, ps_s, ps_r,
):
    z, y, x, t = (lax.axis_index(a) for a in ("z", "y", "x", "tp"))

    def at_z(dz):
        return (lax.rem(z + dz, NZ), y, x, t)

    def at_y(dy):
        return (z, lax.rem(y + dy, NY), x, t)

    def at_x(dx):
        return (z, y, lax.rem(x + dx, NX), t)

    def in_plane(d):
        return (z, lax.rem(y + d // NX, NY), lax.rem(x + d % NX, NX), t)

    def back_in_plane(d):
        return (z, lax.rem(y + NY - d // NX, NY), lax.rem(x + NX - d % NX, NX), t)

    partner = (z, y, x, 1 - t)

    def remote(src, dst, s, r, device):
        return pltpu.make_async_remote_copy(
            src_ref=src, dst_ref=dst, send_sem=s, recv_sem=r, device_id=device, device_id_type=MESH
        )

    barrier = pltpu.get_barrier_semaphore()
    others = [at_z(d) for d in range(1, NZ)] + [in_plane(d) for d in range(1, PLANE)] + [partner]
    for device in others:
        pl.semaphore_signal(barrier, inc=1, device_id=device, device_id_type=MESH)

    loads = []

    def load(src, dst):
        copy = pltpu.make_async_copy(src, dst, load_sem.at[len(loads)])
        copy.start()
        loads.append(copy)
        return copy

    ld_dense = [load(wdg_h, wdg), load(wdu_h, wdu), load(wdd_h, wdd), load(routes_h, routes)]
    ld_tok = [load(tokens_h, tokens), load(attn_gain_h, attn_gain)]
    ld_q = load(wq_h, wq)
    ld_kv = [load(wk_h, wk), load(wv_h, wv)]
    ld_keys = load(keys_h, keys)
    ld_values = load(values_h, values)
    ld_wo = load(wo_h, wo)
    ld_n2 = [load(ffn_gain_h, ffn_gain), load(mix_h, mixw), load(wr_h, wr)]
    ld_eg = [load(weg_h, weg), load(weu_h, weu)]
    ld_ed = [load(wed_h.at[:, pl.ds(h * HALF, HALF)], wed.at[h]) for h in range(2)]

    for copy in ld_dense:
        copy.wait()
    lane = iota((1, NZ * 128), 1)
    first = lax.rem(z + lane // 128, NZ) * 32
    within = lane % 128
    unit = iota((256, NZ * 128), 0)
    eye = bits(iota((ROWS, ROWS), 0) == iota((ROWS, ROWS), 1))
    down_t = dot_nt(eye, wdd[...]).astype(BF16)
    pieces = jnp.zeros((ROWS, NZ * 128), F32)
    for k, w in enumerate((wdg[...], wdu[...], down_t)):
        target = jnp.where((within >= 32 * k) & (within < 32 * k + 32), first + within - 32 * k, -1)
        pieces = pieces + dot(w, bits(unit == target))
    pieces = pieces.astype(BF16)
    for dz in range(NZ):
        w3p[dz] = pieces[:, dz * 128 : (dz + 1) * 128]
    own_hits = jnp.zeros((ROWS, 128), F32)
    for k in range(routes.shape[1]):
        own_hits = own_hits + jnp.where(routes[:, k : k + 1] == iota((ROWS, 128), 1), 1.0, 0.0)
    hits[0] = own_hits.astype(BF16)
    w3[z, y, x] = w3p[0]

    for copy in ld_tok:
        copy.wait()
    normed = rms_scale(tokens[...], attn_gain[...])
    ld_q.wait()
    queries = dot(normed, wq[...]).astype(BF16)
    for copy in ld_kv:
        copy.wait()
    new_keys[...] = dot(normed, wk[...]).astype(BF16)
    new_values[...] = dot(normed, wv[...]).astype(BF16)

    pl.semaphore_wait(barrier, len(others))
    w3z = [remote(w3p.at[d], w3.at[z, y, x], w3z_s.at[d], w3z_r.at[d], at_z(d)) for d in range(1, NZ)]
    hz = [remote(hits.at[0], hits.at[d], h_s.at[d], h_r.at[d], at_z(d)) for d in range(1, NZ)]
    for copy in w3z + hz:
        copy.start()
    w3x = [remote(w3.at[:, y, x], w3.at[:, y, x], w3x_s.at[d], w3x_r.at[d], at_x(d)) for d in range(1, NX)]
    w3y = [remote(w3.at[:, y], w3.at[:, y], w3y_s.at[d], w3y_r.at[d], at_y(d)) for d in range(1, NY)]

    row = iota((128, 1), 0)
    rep = bits(iota((128, ROWS), 0) // 8 == iota((128, ROWS), 1))
    head_lane = iota((128, 512), 1) // 64 == iota((128, 512), 0) % 8
    fold = bits(iota((512, 256), 0) % 64 == iota((512, 256), 1) % 64)
    own_block = iota((128, 256), 1) // 64 == (iota((128, 256), 0) // 8) % 4
    spread = jnp.where(head_lane, dot(rep, queries), 0.0).astype(BF16)
    block_q = jnp.where(own_block, dot(spread, fold), 0.0).astype(BF16)
    bias = jnp.zeros((32, 1), F32)
    for h in range(8):
        bias = jnp.where(iota((32, 1), 0) % 8 == h, head_bias[h], bias)
    after = bits(iota((256, 256), 0) > iota((256, 256), 1))
    ld_keys.wait()
    ld_values.wait()
    mixed = []
    for g in range(4):
        scores = dot(block_q[g * 32 : (g + 1) * 32], keys[pl.ds(g * 256, 256), :]) * 0.125 + bias
        length = jnp.zeros((32, 1), jnp.int32)
        for s in range(4):
            length = jnp.where(iota((32, 1), 0) // 8 == s, lengths[g * 4 + s], length)
        visible = iota((32, 1024), 1) < length
        soft = jnp.log1p(jnp.exp(-jnp.abs(scores)))
        log_take = jnp.minimum(scores, 0.0) - soft
        log_keep = jnp.where(visible, jnp.minimum(-scores, 0.0) - soft, 0.0)
        tiles = jnp.concatenate([log_keep[:, j * 256 : (j + 1) * 256] for j in range(4)], axis=0)
        high, low = two_terms(tiles)
        summed = dot(high, after) + dot(low, after)
        total = summed[:, 0:1] + tiles[:, 0:1]
        later = jnp.zeros((32, 1), F32)
        spans = [None] * 4
        for j in reversed(range(4)):
            spans[j] = summed[j * 32 : (j + 1) * 32] + later
            later = later + total[j * 32 : (j + 1) * 32]
        log_after = jnp.concatenate(spans, axis=1)
        stick = jnp.where(visible, jnp.exp(log_take + log_after), 0.0).astype(BF16)
        mixed.append(dot_nt(stick, values[pl.ds(g * 256, 256), :]))
        if g == 1:
            for copy in w3z:
                copy.wait_recv()
            for copy in w3x:
                copy.start()
        if g == 2:
            for copy in w3x:
                copy.wait_recv()
            for copy in w3y:
                copy.start()
    mixed = jnp.where(own_block, jnp.concatenate(mixed, axis=0), 0.0).astype(BF16)
    unfold = bits(iota((256, 512), 0) % 64 == iota((256, 512), 1) % 64)
    by_head = jnp.where(head_lane, dot(mixed, unfold), 0.0).astype(BF16)
    gather_rows = bits(iota((ROWS, 128), 1) // 8 == iota((ROWS, 128), 0))
    heads_out = dot(gather_rows, by_head).astype(BF16)
    ld_wo.wait()
    part[...] = dot(heads_out, wo[...]).astype(BF16)
    ap = remote(part, peer_part, ap_s.at[0], ap_r.at[0], partner)
    ap.start()

    for copy in hz:
        copy.wait_recv()
    hit = hits[...].reshape(128, 128)
    base = z * PLANE

    def expert_of(slot):
        d = slot // 16
        return base + lax.rem(y + d // NX, NY) * NX + lax.rem(x + d % NX, NX)

    sel = bits(iota((256, 128), 1) == expert_of(iota((256, 128), 0)))
    tok_r, tok_c = iota((128, 128), 0), iota((128, 128), 1)
    earlier_c = bits((tok_r < tok_c) & (tok_r // 16 == tok_c // 16))
    earlier_r = bits((tok_c < tok_r) & (tok_r // 16 == tok_c // 16))
    slot_hit = dot_nt(sel, hit)
    slot_rank = dot(slot_hit.astype(BF16), earlier_c)
    sr, sc = iota((256, 128), 0), iota((256, 128), 1)
    fits = (slot_rank == ((sr // 8) % 2).astype(F32)) & (sc // 16 == sr % 8)
    dispatch = jnp.where(fits, slot_hit, 0.0).astype(BF16)
    tok_hit = dot_nt(hit, sel)
    tok_rank = dot_nt(dot(earlier_r, hit).astype(BF16), sel)
    cr, cc = iota((128, 256), 0), iota((128, 256), 1)
    taken = (tok_rank == ((cc // 8) % 2).astype(F32)) & (cr // 16 == cc % 8) & (tok_hit > 0.5)

    for copy in ld_n2:
        copy.wait()
    ap.wait_recv()
    residual = (tokens[...].astype(F32) + (part[...].astype(F32) + peer_part[...].astype(F32))).astype(BF16)
    normed2 = rms_scale(residual, ffn_gain[...])
    for h in range(2):
        norm2[h] = normed2[:, h * HALF : (h + 1) * HALF]
        resid[h] = residual[:, h * HALF : (h + 1) * HALF]
    tokf[t, 0] = norm2[t]
    tz = [remote(norm2.at[t], tokf.at[t, d], tz_s.at[d], tz_r.at[d], at_z(d)) for d in range(1, NZ)]
    for d in (4, 3, 5, 2, 6, 1, 7):
        tz[d - 1].start()
    probs = sigmoid(dot(normed2, wr[...]))
    picked = own_hits * probs
    gates = picked / jnp.sum(picked, axis=-1, keepdims=True) * 2.5
    mix = sigmoid(jnp.sum(normed2.astype(F32) * mixw[...], axis=-1, keepdims=True))
    gm[0] = jnp.concatenate([gates, jnp.broadcast_to(mix, (ROWS, 128))], axis=1)
    gz = [remote(gm.at[0], gm.at[d], g_s.at[d], g_r.at[d], at_z(d)) for d in range(1, NZ)]
    for copy in gz:
        copy.start()

    for copy in tz:
        copy.wait_recv()
    rows = dot(dispatch, tokf[t].reshape(128, HALF)).astype(BF16).reshape(PLANE, 16, HALF)
    for d in range(1, PLANE):
        xs[d] = rows[d]
    xin[t, 0] = rows[0]
    xd = [remote(xs.at[d], xin.at[t, d], xs_s.at[d], xs_r.at[d], in_plane(d)) for d in range(1, PLANE)]
    order = sorted(range(1, PLANE), key=lambda d: -(min(d // NX, NY - d // NX) + min(d % NX, NX - d % NX)))
    for d in order:
        xd[d - 1].start()
    tf = remote(tokf.at[t], tokf.at[t], tf_s.at[0], tf_r.at[0], partner)
    tf.start()
    xf = [remote(xin.at[t, d], xin.at[t, d], xf_s.at[d], xf_r.at[d], partner) for d in range(PLANE)]
    xf[0].start()

    for copy in w3y:
        copy.wait_recv()
    tf.wait_recv()
    lo, hi = w3[0:4].reshape(HALF, 128), w3[4:8].reshape(HALF, 128)
    pre = dot(tokf[0].reshape(128, HALF), lo) + dot(tokf[1].reshape(128, HALF), hi)
    gate_in, up_in = pltpu.roll(pre, 64, 1), pltpu.roll(pre, 32, 1)
    used = (iota((128, 128), 1) >= 64) & (iota((128, 128), 1) < 96)
    dense_hidden = jnp.where(used, gate_in * sigmoid(gate_in) * up_in, 0.0).astype(BF16)
    dn_send[...] = dot_nt(dense_hidden, w3[pl.ds(4 * (1 - t), 4)].reshape(HALF, 128)).astype(BF16)
    dn = remote(dn_send, dn_peer, dn_s.at[0], dn_r.at[0], partner)
    dn.start()
    dn_mine[...] = dot_nt(dense_hidden, w3[pl.ds(4 * t, 4)].reshape(HALF, 128)).astype(BF16)

    for d in reversed(order):
        xd[d - 1].wait_recv()
        xf[d].start()
    for copy in ld_eg:
        copy.wait()
    mine = xin[t].reshape(256, HALF)
    gate_mine = dot(mine, weg[t])
    up_mine = dot(mine, weu[t])
    for copy in xf:
        copy.wait_recv()
    theirs = xin[1 - t].reshape(256, HALF)
    gate_rows = gate_mine + dot(theirs, weg[1 - t])
    up_rows = up_mine + dot(theirs, weu[1 - t])
    hidden = (gate_rows * sigmoid(gate_rows) * up_rows).astype(BF16)
    for copy in ld_ed:
        copy.wait()
    eo_send[...] = dot(hidden, wed[1 - t]).astype(BF16)
    eo = remote(eo_send, eo_peer, eo_s.at[0], eo_r.at[0], partner)
    eo.start()
    eo_mine[...] = dot(hidden, wed[t]).astype(BF16)

    for copy in gz:
        copy.wait_recv()
    gmv = gm[...].reshape(128, 256)
    gate_high, gate_low = two_terms(gmv[:, 0:128])
    slot_gate = jnp.where(taken, dot_nt(gate_high, sel) + dot_nt(gate_low, sel), 0.0)
    comb_high, comb_low = two_terms(slot_gate)
    dn.wait_recv()
    dense = gmv[:, 128:129] * (dn_mine[...].astype(F32) + dn_peer[...].astype(F32))

    eo.wait_recv()
    done = (eo_mine[...].astype(F32) + eo_peer[...].astype(F32)).astype(BF16).reshape(PLANE, 16, HALF)
    for d in range(1, PLANE):
        ys[d] = done[d]
    yr[0] = done[0]
    yd = [remote(ys.at[d], yr.at[d], ys_s.at[d], ys_r.at[d], back_in_plane(d)) for d in range(1, PLANE)]
    for d in order:
        yd[d - 1].start()
    for copy in yd:
        copy.wait_recv()
    back = yr[...].reshape(256, HALF)
    sums = dense + (dot(comb_high, back) + dot(comb_low, back))
    sums3 = sums.astype(BF16).reshape(NZ, ROWS, HALF)
    for d in range(1, NZ):
        ps[d] = sums3[d]
    zd = [
        remote(ps.at[d], pr.at[d], ps_s.at[d], ps_r.at[d], at_z(NZ - d)) for d in range(1, NZ)
    ]
    for d in (4, 3, 5, 2, 6, 1, 7):
        zd[d - 1].start()
    total_out = resid[t].astype(F32) + sums[0:ROWS]
    for copy in zd:
        copy.wait_recv()
    for d in range(1, NZ):
        total_out = total_out + pr[d].astype(F32)
    out[...] = total_out.astype(BF16)
    for copy in [*w3z, *hz, *w3x, *w3y, ap, *tz, *gz, tf, *xd, *xf, dn, eo, *yd, *zd]:
        copy.wait_send()


def shards(
    tokens, lengths, attn_gain, w_query, w_key, w_value, head_bias, key_cache, value_cache, w_attn_out,
    ffn_gain, w_router, routes, w_dense_gate, w_dense_up, w_dense_down, dense_mix,
    w_expert_gate, w_expert_up, w_expert_down,
):
    args = (
        tokens, lengths, attn_gain.reshape(1, WIDTH), w_query, w_key, w_value, head_bias,
        key_cache.reshape(1024, 1024), value_cache.reshape(1024, 1024), w_attn_out,
        ffn_gain.reshape(1, WIDTH), w_router, routes, w_dense_gate, w_dense_up, w_dense_down,
        dense_mix.reshape(1, WIDTH), w_expert_gate.reshape(2, HALF, 256), w_expert_up.reshape(2, HALF, 256),
        w_expert_down.reshape(256, WIDTH),
    )
    smem = {1, 6}
    vm, dma = pltpu.VMEM, pltpu.SemaphoreType.DMA
    scratch = [
        vm((ROWS, WIDTH), BF16), vm((1, WIDTH), F32), vm((WIDTH, 512), BF16), vm((WIDTH, 64), BF16),
        vm((WIDTH, 64), BF16), vm((1024, 1024), BF16), vm((1024, 1024), BF16), vm((512, WIDTH), BF16),
        vm((1, WIDTH), F32), vm((WIDTH, 128), BF16), vm((ROWS, 6), jnp.int32), vm((ROWS, 256), BF16),
        vm((ROWS, 256), BF16), vm((256, ROWS), BF16), vm((1, WIDTH), F32),
        vm((2, HALF, 256), BF16), vm((2, HALF, 256), BF16), vm((2, 256, HALF), BF16),
        vm((NZ, ROWS, 128), BF16), vm((NZ, NY, NX, ROWS, 128), BF16), vm((NZ, ROWS, 128), BF16),
        vm((NZ, ROWS, 256), F32), vm((ROWS, WIDTH), BF16), vm((ROWS, WIDTH), BF16),
        vm((2, ROWS, HALF), BF16), vm((2, ROWS, HALF), BF16), vm((2, NZ, ROWS, HALF), BF16),
        vm((PLANE, 16, HALF), BF16), vm((2, PLANE, 16, HALF), BF16),
        vm((256, HALF), BF16), vm((256, HALF), BF16), vm((256, HALF), BF16),
        vm((PLANE, 16, HALF), BF16), vm((PLANE, 16, HALF), BF16),
        vm((128, HALF), BF16), vm((128, HALF), BF16), vm((128, HALF), BF16),
        vm((NZ, ROWS, HALF), BF16), vm((NZ, ROWS, HALF), BF16),
        dma((LOADS,)),
    ]
    for n in (NZ, NX, NY, NZ, 1, NZ, NZ, 1, PLANE, PLANE, 1, PLANE, 1, NZ):
        scratch += [dma((n,)), dma((n,))]
    return pl.pallas_call(
        kernel,
        out_shape=(
            jax.ShapeDtypeStruct((ROWS, HALF), BF16),
            jax.ShapeDtypeStruct((ROWS, 64), BF16),
            jax.ShapeDtypeStruct((ROWS, 64), BF16),
        ),
        in_specs=[
            pl.BlockSpec(memory_space=pltpu.SMEM if k in smem else pl.ANY) for k in range(len(args))
        ],
        out_specs=tuple(pl.BlockSpec(memory_space=pltpu.VMEM) for _ in range(3)),
        scratch_shapes=scratch,
        compiler_params=pltpu.CompilerParams(
            collective_id=0, has_side_effects=True, vmem_limit_bytes=60 * 1024 * 1024
        ),
    )(*args)


def solution(mesh):
    finer = Mesh(mesh.devices.reshape(NZ, NY, NX, mesh.shape["tp"]), ("z", "y", "x", "tp"))
    placed = (
        P(EP, None), P(EP), P(), P(None, "tp"), P(None, "tp"), P(None, "tp"), P("tp"),
        P(EP, "tp", None, None), P(EP, "tp", None, None), P("tp", None), P(), P(), P(EP, None),
        P(EP, "tp"), P(EP, "tp"), P("tp", EP), P(), P(EP, None, "tp"), P(EP, None, "tp"), P(EP, "tp", None),
    )
    return jax.shard_map(
        shards, mesh=finer, in_specs=placed, out_specs=(P(EP, "tp"), P(EP, "tp"), P(EP, "tp")), check_vma=False
    )
```

```python
import jax
import jax.numpy as jnp
from jax import lax
from jax.experimental import pallas as pl
from jax.experimental.pallas import tpu as pltpu
from jax.sharding import Mesh
from jax.sharding import PartitionSpec as P

EP = ("z", "y", "x")
MESH = pl.DeviceIdType.MESH
NZ, NY, NX = 8, 4, 4
PLANE = NY * NX
ROWS, WIDTH, HALF = 16, 2048, 1024
F32, BF16 = jnp.float32, jnp.bfloat16
NT = (((1,), (1,)), ((), ()))
LOADS = 21


def dot(a, b):
    return jnp.dot(a, b, preferred_element_type=F32)


def dot_nt(a, b):
    return lax.dot_general(a, b, NT, preferred_element_type=F32)


def iota(shape, dim):
    return lax.broadcasted_iota(jnp.int32, shape, dim)


def bits(mask):
    return jnp.where(mask, 1.0, 0.0).astype(BF16)


def two_terms(x):
    high = x.astype(BF16)
    return high, (x - high.astype(F32)).astype(BF16)


def sigmoid(x):
    return 1.0 / (1.0 + jnp.exp(-x))


def rms_scale(values, gain):
    wide = values.astype(F32)
    return (wide * lax.rsqrt(jnp.mean(wide * wide, axis=-1, keepdims=True) + 1e-06) * gain).astype(BF16)


def kernel(
    tokens_h, lengths, attn_gain_h, wq_h, wk_h, wv_h, head_bias, keys_h, values_h, wo_h,
    ffn_gain_h, wr_h, routes_h, wdg_h, wdu_h, wdd_h, mix_h, weg_h, weu_h, wed_h,
    out, new_keys, new_values,
    tokens, attn_gain, wq, wk, wv, keys, values, wo, ffn_gain, wr, routes, wdg, wdu, wdd, mixw,
    weg, weu, wed,
    w3p, w3, hits, gm, part, peer_part, norm2, resid, tokf, xs, xin, eo_mine, eo_send, eo_peer,
    ys, yr, dn_mine, dn_send, dn_peer, ps, pr,
    load_sem, w3z_s, w3z_r, w3x_s, w3x_r, w3y_s, w3y_r, h_s, h_r, ap_s, ap_r, tz_s, tz_r, g_s, g_r,
    tf_s, tf_r, xs_s, xs_r, xf_s, xf_r, eo_s, eo_r, ys_s, ys_r, dn_s, dn_r, ps_s, ps_r,
):
    scope = []

    def stage(name=None):
        if scope:
            scope.pop().__exit__(None, None, None)
        if name:
            scope.append(jax.named_scope(name))
            scope[0].__enter__()

    stage("enter")
    z, y, x, t = (lax.axis_index(a) for a in ("z", "y", "x", "tp"))

    def at_z(dz):
        return (lax.rem(z + dz, NZ), y, x, t)

    def at_y(dy):
        return (z, lax.rem(y + dy, NY), x, t)

    def at_x(dx):
        return (z, y, lax.rem(x + dx, NX), t)

    def in_plane(d):
        return (z, lax.rem(y + d // NX, NY), lax.rem(x + d % NX, NX), t)

    def back_in_plane(d):
        return (z, lax.rem(y + NY - d // NX, NY), lax.rem(x + NX - d % NX, NX), t)

    partner = (z, y, x, 1 - t)

    def remote(src, dst, s, r, device):
        return pltpu.make_async_remote_copy(
            src_ref=src, dst_ref=dst, send_sem=s, recv_sem=r, device_id=device, device_id_type=MESH
        )

    barrier = pltpu.get_barrier_semaphore()
    others = [at_z(d) for d in range(1, NZ)] + [in_plane(d) for d in range(1, PLANE)] + [partner]
    for device in others:
        pl.semaphore_signal(barrier, inc=1, device_id=device, device_id_type=MESH)

    loads = []

    def load(src, dst):
        copy = pltpu.make_async_copy(src, dst, load_sem.at[len(loads)])
        copy.start()
        loads.append(copy)
        return copy

    ld_dense = [load(wdg_h, wdg), load(wdu_h, wdu), load(wdd_h, wdd), load(routes_h, routes)]
    ld_tok = [load(tokens_h, tokens), load(attn_gain_h, attn_gain)]
    ld_q = load(wq_h, wq)
    ld_kv = [load(wk_h, wk), load(wv_h, wv)]
    ld_keys = load(keys_h, keys)
    ld_values = load(values_h, values)
    ld_wo = load(wo_h, wo)
    ld_n2 = [load(ffn_gain_h, ffn_gain), load(mix_h, mixw), load(wr_h, wr)]
    ld_eg = [load(weg_h, weg), load(weu_h, weu)]
    ld_ed = [load(wed_h.at[:, pl.ds(h * HALF, HALF)], wed.at[h]) for h in range(2)]

    stage("dense_slices")
    for copy in ld_dense:
        copy.wait()
    lane = iota((1, NZ * 128), 1)
    first = lax.rem(z + lane // 128, NZ) * 32
    within = lane % 128
    unit = iota((256, NZ * 128), 0)
    pieces = jnp.zeros((ROWS, NZ * 128), F32)
    for k, w in enumerate((wdg[...], wdu[...], wdd[...])):
        target = jnp.where((within >= 32 * k) & (within < 32 * k + 32), first + within - 32 * k, -1)
        pieces = pieces + dot(w, bits(unit == target))
    pieces = pieces.astype(BF16)
    for dz in range(NZ):
        w3p[dz] = pieces[:, dz * 128 : (dz + 1) * 128]
    hits_t = jnp.zeros((128, ROWS), F32)
    for k in range(routes.shape[0]):
        hits_t = hits_t + jnp.where(routes[k : k + 1, :] == iota((128, ROWS), 0), 1.0, 0.0)
    eye = bits(iota((ROWS, ROWS), 0) == iota((ROWS, ROWS), 1))
    own_hits = dot_nt(eye, hits_t.astype(BF16))
    hits[0] = own_hits.astype(BF16)
    w3[z, y, x] = w3p[0]

    stage("project")
    for copy in ld_tok:
        copy.wait()
    normed = rms_scale(tokens[...], attn_gain[...])
    ld_q.wait()
    queries = dot(normed, wq[...]).astype(BF16)
    for copy in ld_kv:
        copy.wait()
    new_keys[...] = dot_nt(normed, wk[...]).astype(BF16)
    new_values[...] = dot_nt(normed, wv[...]).astype(BF16)

    stage("barrier")
    pl.semaphore_wait(barrier, len(others))
    w3z = [remote(w3p.at[d], w3.at[z, y, x], w3z_s.at[d], w3z_r.at[d], at_z(d)) for d in range(1, NZ)]
    hz = [remote(hits.at[0], hits.at[d], h_s.at[d], h_r.at[d], at_z(d)) for d in range(1, NZ)]
    for copy in w3z + hz:
        copy.start()
    w3x = [remote(w3.at[:, y, x], w3.at[:, y, x], w3x_s.at[d], w3x_r.at[d], at_x(d)) for d in range(1, NX)]
    w3y = [remote(w3.at[:, y], w3.at[:, y], w3y_s.at[d], w3y_r.at[d], at_y(d)) for d in range(1, NY)]

    stage("attention")
    row = iota((128, 1), 0)
    rep = bits(iota((128, ROWS), 0) // 8 == iota((128, ROWS), 1))
    head_lane = iota((128, 512), 1) // 64 == iota((128, 512), 0) % 8
    fold = bits(iota((512, 256), 0) % 64 == iota((512, 256), 1) % 64)
    own_block = iota((128, 256), 1) // 64 == (iota((128, 256), 0) // 8) % 4
    spread = jnp.where(head_lane, dot(rep, queries), 0.0).astype(BF16)
    block_q = jnp.where(own_block, dot(spread, fold), 0.0).astype(BF16)
    bias = jnp.zeros((32, 1), F32)
    for h in range(8):
        bias = jnp.where(iota((32, 1), 0) % 8 == h, head_bias[h], bias)
    after = bits(iota((256, 256), 0) > iota((256, 256), 1))
    ld_keys.wait()
    ld_values.wait()
    mixed = []
    for g in range(4):
        scores = dot(block_q[g * 32 : (g + 1) * 32], keys[pl.ds(g * 256, 256), :]) * 0.125 + bias
        length = jnp.zeros((32, 1), jnp.int32)
        for s in range(4):
            length = jnp.where(iota((32, 1), 0) // 8 == s, lengths[g * 4 + s], length)
        visible = iota((32, 1024), 1) < length
        soft = jnp.log1p(jnp.exp(-jnp.abs(scores)))
        log_take = jnp.minimum(scores, 0.0) - soft
        log_keep = jnp.where(visible, jnp.minimum(-scores, 0.0) - soft, 0.0)
        tiles = jnp.concatenate([log_keep[:, j * 256 : (j + 1) * 256] for j in range(4)], axis=0)
        high, low = two_terms(tiles)
        summed = dot(high, after) + dot(low, after)
        total = summed[:, 0:1] + tiles[:, 0:1]
        later = jnp.zeros((32, 1), F32)
        spans = [None] * 4
        for j in reversed(range(4)):
            spans[j] = summed[j * 32 : (j + 1) * 32] + later
            later = later + total[j * 32 : (j + 1) * 32]
        log_after = jnp.concatenate(spans, axis=1)
        stick = jnp.where(visible, jnp.exp(log_take + log_after), 0.0).astype(BF16)
        mixed.append(dot_nt(stick, values[pl.ds(g * 256, 256), :]))
        if g == 1:
            for copy in w3z:
                copy.wait_recv()
            for copy in w3x:
                copy.start()
        if g == 2:
            for copy in w3x:
                copy.wait_recv()
            for copy in w3y:
                copy.start()
    mixed = jnp.where(own_block, jnp.concatenate(mixed, axis=0), 0.0).astype(BF16)
    unfold = bits(iota((256, 512), 0) % 64 == iota((256, 512), 1) % 64)
    by_head = jnp.where(head_lane, dot(mixed, unfold), 0.0).astype(BF16)
    gather_rows = bits(iota((ROWS, 128), 1) // 8 == iota((ROWS, 128), 0))
    heads_out = dot(gather_rows, by_head).astype(BF16)
    stage("attention_out")
    ld_wo.wait()
    part[...] = dot(heads_out, wo[...]).astype(BF16)
    ap = remote(part, peer_part, ap_s.at[0], ap_r.at[0], partner)
    ap.start()

    stage("slots")
    for copy in hz:
        copy.wait_recv()
    hit = hits[...].reshape(128, 128)
    base = z * PLANE

    def expert_of(slot):
        d = slot // 16
        return base + lax.rem(y + d // NX, NY) * NX + lax.rem(x + d % NX, NX)

    sel = bits(iota((256, 128), 1) == expert_of(iota((256, 128), 0)))
    tok_r, tok_c = iota((128, 128), 0), iota((128, 128), 1)
    earlier_c = bits((tok_r < tok_c) & (tok_r // 16 == tok_c // 16))
    earlier_r = bits((tok_c < tok_r) & (tok_r // 16 == tok_c // 16))
    slot_hit = dot_nt(sel, hit)
    slot_rank = dot(slot_hit.astype(BF16), earlier_c)
    sr, sc = iota((256, 128), 0), iota((256, 128), 1)
    fits = (slot_rank == ((sr // 8) % 2).astype(F32)) & (sc // 16 == sr % 8)
    dispatch = jnp.where(fits, slot_hit, 0.0).astype(BF16)
    tok_hit = dot_nt(hit, sel)
    tok_rank = dot_nt(dot(earlier_r, hit).astype(BF16), sel)
    cr, cc = iota((128, 256), 0), iota((128, 256), 1)
    taken = (tok_rank == ((cc // 8) % 2).astype(F32)) & (cr // 16 == cc % 8) & (tok_hit > 0.5)

    stage("core_sum")
    for copy in ld_n2:
        copy.wait()
    ap.wait_recv()
    residual = (tokens[...].astype(F32) + (part[...].astype(F32) + peer_part[...].astype(F32))).astype(BF16)
    normed2 = rms_scale(residual, ffn_gain[...])
    for h in range(2):
        norm2[h] = normed2[:, h * HALF : (h + 1) * HALF]
        resid[h] = residual[:, h * HALF : (h + 1) * HALF]
    tokf[t, 0] = norm2[t]
    tz = [remote(norm2.at[t], tokf.at[t, d], tz_s.at[d], tz_r.at[d], at_z(d)) for d in range(1, NZ)]
    for d in (4, 3, 5, 2, 6, 1, 7):
        tz[d - 1].start()
    stage("router")
    probs = sigmoid(dot(normed2, wr[...]))
    picked = own_hits * probs
    gates = picked / jnp.sum(picked, axis=-1, keepdims=True) * 2.5
    mix = sigmoid(jnp.sum(normed2.astype(F32) * mixw[...], axis=-1, keepdims=True))
    gm[0] = jnp.concatenate([gates, jnp.broadcast_to(mix, (ROWS, 128))], axis=1)
    gz = [remote(gm.at[0], gm.at[d], g_s.at[d], g_r.at[d], at_z(d)) for d in range(1, NZ)]
    for copy in gz:
        copy.start()

    stage("z_gather")
    for copy in tz:
        copy.wait_recv()
    stage("dispatch")
    rows = dot(dispatch, tokf[t].reshape(128, HALF)).astype(BF16).reshape(PLANE, 16, HALF)
    for d in range(1, PLANE):
        xs[d] = rows[d]
    xin[t, 0] = rows[0]
    xd = [remote(xs.at[d], xin.at[t, d], xs_s.at[d], xs_r.at[d], in_plane(d)) for d in range(1, PLANE)]
    order = sorted(range(1, PLANE), key=lambda d: -(min(d // NX, NY - d // NX) + min(d % NX, NX - d % NX)))
    for d in order:
        xd[d - 1].start()
    tf = remote(tokf.at[t], tokf.at[t], tf_s.at[0], tf_r.at[0], partner)
    tf.start()
    xf = [remote(xin.at[t, d], xin.at[t, d], xf_s.at[d], xf_r.at[d], partner) for d in range(PLANE)]
    xf[0].start()

    stage("dense")
    for copy in w3y:
        copy.wait_recv()
    tf.wait_recv()
    lo, hi = w3[0:4].reshape(HALF, 128), w3[4:8].reshape(HALF, 128)
    pre = dot(tokf[0].reshape(128, HALF), lo) + dot(tokf[1].reshape(128, HALF), hi)
    gate_in, up_in = pltpu.roll(pre, 64, 1), pltpu.roll(pre, 32, 1)
    used = (iota((128, 128), 1) >= 64) & (iota((128, 128), 1) < 96)
    dense_hidden = jnp.where(used, gate_in * sigmoid(gate_in) * up_in, 0.0).astype(BF16)
    dn_send[...] = dot_nt(dense_hidden, w3[pl.ds(4 * (1 - t), 4)].reshape(HALF, 128)).astype(BF16)
    dn = remote(dn_send, dn_peer, dn_s.at[0], dn_r.at[0], partner)
    dn.start()
    dn_mine[...] = dot_nt(dense_hidden, w3[pl.ds(4 * t, 4)].reshape(HALF, 128)).astype(BF16)

    stage("plane_in")
    for d in reversed(order):
        xd[d - 1].wait_recv()
        xf[d].start()
    for copy in ld_eg:
        copy.wait()
    stage("expert_own")
    mine = xin[t].reshape(256, HALF)
    gate_mine = dot(mine, weg[t])
    up_mine = dot(mine, weu[t])
    stage("forward_wait")
    for copy in xf:
        copy.wait_recv()
    stage("expert")
    theirs = xin[1 - t].reshape(256, HALF)
    gate_rows = gate_mine + dot(theirs, weg[1 - t])
    up_rows = up_mine + dot(theirs, weu[1 - t])
    hidden = (gate_rows * sigmoid(gate_rows) * up_rows).astype(BF16)
    for copy in ld_ed:
        copy.wait()
    eo_send[...] = dot(hidden, wed[1 - t]).astype(BF16)
    eo = remote(eo_send, eo_peer, eo_s.at[0], eo_r.at[0], partner)
    eo.start()
    eo_mine[...] = dot(hidden, wed[t]).astype(BF16)

    stage("gates")
    for copy in gz:
        copy.wait_recv()
    gmv = gm[...].reshape(128, 256)
    gate_high, gate_low = two_terms(gmv[:, 0:128])
    slot_gate = jnp.where(taken, dot_nt(gate_high, sel) + dot_nt(gate_low, sel), 0.0)
    comb_high, comb_low = two_terms(slot_gate)
    dn.wait_recv()
    dense = gmv[:, 128:129] * (dn_mine[...].astype(F32) + dn_peer[...].astype(F32))

    stage("expert_sum")
    eo.wait_recv()
    done = (eo_mine[...].astype(F32) + eo_peer[...].astype(F32)).astype(BF16).reshape(PLANE, 16, HALF)
    for d in range(1, PLANE):
        ys[d] = done[d]
    yr[0] = done[0]
    stage("plane_send")
    yd = [remote(ys.at[d], yr.at[d], ys_s.at[d], ys_r.at[d], back_in_plane(d)) for d in range(1, PLANE)]
    for d in order:
        yd[d - 1].start()
    stage("plane_back")
    for copy in yd:
        copy.wait_recv()
    stage("combine")
    back = yr[...].reshape(256, HALF)
    sums = dense + (dot(comb_high, back) + dot(comb_low, back))
    sums3 = sums.astype(BF16).reshape(NZ, ROWS, HALF)
    for d in range(1, NZ):
        ps[d] = sums3[d]
    zd = [
        remote(ps.at[d], pr.at[d], ps_s.at[d], ps_r.at[d], at_z(NZ - d)) for d in range(1, NZ)
    ]
    for d in (4, 3, 5, 2, 6, 1, 7):
        zd[d - 1].start()
    stage("z_wait")
    total_out = resid[t].astype(F32) + sums[0:ROWS]
    for copy in zd:
        copy.wait_recv()
    stage("finish")
    for d in range(1, NZ):
        total_out = total_out + pr[d].astype(F32)
    out[...] = total_out.astype(BF16)
    for copy in [*w3z, *hz, *w3x, *w3y, ap, *tz, *gz, tf, *xd, *xf, dn, eo, *yd, *zd]:
        copy.wait_send()
    stage()


def hand_over(*refs):
    for k in range(3):
        refs[3 + k][...] = refs[k][...]


def shards(
    tokens, lengths, attn_gain, w_query, w_key, w_value, head_bias, key_cache, value_cache, w_attn_out,
    ffn_gain, w_router, routes, w_dense_gate, w_dense_up, w_dense_down, dense_mix,
    w_expert_gate, w_expert_up, w_expert_down,
):
    args = (
        tokens, lengths, attn_gain.reshape(1, WIDTH), w_query, w_key.T, w_value.T, head_bias,
        key_cache.reshape(1024, 1024), value_cache.reshape(1024, 1024), w_attn_out,
        ffn_gain.reshape(1, WIDTH), w_router, routes.T, w_dense_gate, w_dense_up, w_dense_down.T,
        dense_mix.reshape(1, WIDTH), w_expert_gate.reshape(2, HALF, 256), w_expert_up.reshape(2, HALF, 256),
        w_expert_down.reshape(256, WIDTH),
    )
    smem = {1, 6}
    vm, dma = pltpu.VMEM, pltpu.SemaphoreType.DMA
    scratch = [
        vm((ROWS, WIDTH), BF16), vm((1, WIDTH), F32), vm((WIDTH, 512), BF16), vm((64, WIDTH), BF16),
        vm((64, WIDTH), BF16), vm((1024, 1024), BF16), vm((1024, 1024), BF16), vm((512, WIDTH), BF16),
        vm((1, WIDTH), F32), vm((WIDTH, 128), BF16), vm((6, ROWS), jnp.int32), vm((ROWS, 256), BF16),
        vm((ROWS, 256), BF16), vm((ROWS, 256), BF16), vm((1, WIDTH), F32),
        vm((2, HALF, 256), BF16), vm((2, HALF, 256), BF16), vm((2, 256, HALF), BF16),
        vm((NZ, ROWS, 128), BF16), vm((NZ, NY, NX, ROWS, 128), BF16), vm((NZ, ROWS, 128), BF16),
        vm((NZ, ROWS, 256), F32), vm((ROWS, WIDTH), BF16), vm((ROWS, WIDTH), BF16),
        vm((2, ROWS, HALF), BF16), vm((2, ROWS, HALF), BF16), vm((2, NZ, ROWS, HALF), BF16),
        vm((PLANE, 16, HALF), BF16), vm((2, PLANE, 16, HALF), BF16),
        vm((256, HALF), BF16), vm((256, HALF), BF16), vm((256, HALF), BF16),
        vm((PLANE, 16, HALF), BF16), vm((PLANE, 16, HALF), BF16),
        vm((128, HALF), BF16), vm((128, HALF), BF16), vm((128, HALF), BF16),
        vm((NZ, ROWS, HALF), BF16), vm((NZ, ROWS, HALF), BF16),
        dma((LOADS,)),
    ]
    for n in (NZ, NX, NY, NZ, 1, NZ, NZ, 1, PLANE, PLANE, 1, PLANE, 1, NZ):
        scratch += [dma((n,)), dma((n,))]
    results = pl.pallas_call(
        kernel,
        out_shape=(
            jax.ShapeDtypeStruct((ROWS, HALF), BF16),
            jax.ShapeDtypeStruct((ROWS, 64), BF16),
            jax.ShapeDtypeStruct((ROWS, 64), BF16),
        ),
        in_specs=[
            pl.BlockSpec(memory_space=pltpu.SMEM if k in smem else pl.ANY) for k in range(len(args))
        ],
        out_specs=tuple(pl.BlockSpec(memory_space=pltpu.VMEM) for _ in range(3)),
        scratch_shapes=scratch,
        compiler_params=pltpu.CompilerParams(
            collective_id=0, has_side_effects=True, vmem_limit_bytes=60 * 1024 * 1024
        ),
    )(*args)
    whole = pl.BlockSpec(memory_space=pltpu.VMEM)
    return pl.pallas_call(
        hand_over,
        out_shape=tuple(jax.ShapeDtypeStruct(r.shape, r.dtype) for r in results),
        in_specs=[whole] * 3,
        out_specs=(whole,) * 3,
    )(*results)


def solution(mesh):
    finer = Mesh(mesh.devices.reshape(NZ, NY, NX, mesh.shape["tp"]), ("z", "y", "x", "tp"))
    placed = (
        P(EP, None), P(EP), P(), P(None, "tp"), P(None, "tp"), P(None, "tp"), P("tp"),
        P(EP, "tp", None, None), P(EP, "tp", None, None), P("tp", None), P(), P(), P(EP, None),
        P(EP, "tp"), P(EP, "tp"), P("tp", EP), P(), P(EP, None, "tp"), P(EP, None, "tp"), P(EP, "tp", None),
    )
    return jax.shard_map(
        shards, mesh=finer, in_specs=placed, out_specs=(P(EP, "tp"), P(EP, "tp"), P(EP, "tp")), check_vma=False
    )
```

```python
import jax
import jax.numpy as jnp
from jax import lax
from jax.experimental import pallas as pl
from jax.experimental.pallas import tpu as pltpu
from jax.sharding import Mesh
from jax.sharding import PartitionSpec as P

EP = ("z", "y", "x")
MESH = pl.DeviceIdType.MESH
NZ, NY, NX = 8, 4, 4
PLANE = NY * NX
ROWS, WIDTH, HALF = 16, 2048, 1024
F32, BF16 = jnp.float32, jnp.bfloat16
NT = (((1,), (1,)), ((), ()))
LOADS = 21
CHUNKS = 4
WIDE = HALF // CHUNKS
FAR_Z = (4, 3, 5, 2, 6, 1, 7)


def dot(a, b):
    return jnp.dot(a, b, preferred_element_type=F32)


def dot_nt(a, b):
    return lax.dot_general(a, b, NT, preferred_element_type=F32)


def iota(shape, dim):
    return lax.broadcasted_iota(jnp.int32, shape, dim)


def bits(mask):
    return jnp.where(mask, 1.0, 0.0).astype(BF16)


def two_terms(x):
    high = x.astype(BF16)
    return high, (x - high.astype(F32)).astype(BF16)


def sigmoid(x):
    return 1.0 / (1.0 + jnp.exp(-x))


def rms_scale(values, gain):
    wide = values.astype(F32)
    return (wide * lax.rsqrt(jnp.mean(wide * wide, axis=-1, keepdims=True) + 1e-06) * gain).astype(BF16)


def kernel(
    tokens_h, lengths, attn_gain_h, wq_h, wk_h, wv_h, head_bias, keys_h, values_h, wo_h,
    ffn_gain_h, wr_h, routes_h, wdg_h, wdu_h, wdd_h, mix_h, weg_h, weu_h, wed_h,
    out_h, new_keys_h, new_values_h, out, new_keys, new_values,
    tokens, attn_gain, wq, wk, wv, keys, values, wo, ffn_gain, wr, routes, wdg, wdu, wdd, mixw,
    weg, weu, wed,
    w3p, w3, hits, part, peer_part, norm2, resid, tokf, xs, xin, eo_mine, eo_send, eo_peer,
    ys, yr, dn_mine, dn_send, dn_peer, ps, pr,
    load_sem, store_sem, w3z_s, w3z_r, w3a_s, w3a_r, w3b_s, w3b_r, h_s, h_r, ap_s, ap_r, tz_s, tz_r,
    tf_s, tf_r, xs_s, xs_r, xf_s, xf_r, eo_s, eo_r, ys_s, ys_r, dn_s, dn_r, ps_s, ps_r,
):
    scope = []

    def stage(name=None):
        if scope:
            scope.pop().__exit__(None, None, None)
        if name:
            scope.append(jax.named_scope(name))
            scope[0].__enter__()

    stage("enter")
    z, y, x, t = (lax.axis_index(a) for a in ("z", "y", "x", "tp"))

    def at_z(dz):
        return (lax.rem(z + dz, NZ), y, x, t)

    def at_y(dy):
        return (z, lax.rem(y + dy, NY), x, t)

    def at_x(dx):
        return (z, y, lax.rem(x + dx, NX), t)

    def in_plane(d):
        return (z, lax.rem(y + d // NX, NY), lax.rem(x + d % NX, NX), t)

    def back_in_plane(d):
        return (z, lax.rem(y + NY - d // NX, NY), lax.rem(x + NX - d % NX, NX), t)

    partner = (z, y, x, 1 - t)

    def remote(src, dst, s, r, device):
        return pltpu.make_async_remote_copy(
            src_ref=src, dst_ref=dst, send_sem=s, recv_sem=r, device_id=device, device_id_type=MESH
        )

    def settle(like, sem):
        pltpu.make_async_copy(like, like, sem).wait()

    barrier = pltpu.get_barrier_semaphore()
    others = [at_z(d) for d in range(1, NZ)] + [in_plane(d) for d in range(1, PLANE)] + [partner]
    for device in others:
        pl.semaphore_signal(barrier, inc=1, device_id=device, device_id_type=MESH)

    loads = []

    def load(src, dst):
        copy = pltpu.make_async_copy(src, dst, load_sem.at[len(loads)])
        copy.start()
        loads.append(copy)
        return copy

    ld_dense = [load(routes_h, routes)]
    ld_tok = [load(tokens_h, tokens), load(attn_gain_h, attn_gain)]
    ld_q = load(wq_h, wq)
    ld_kv = [load(wk_h, wk), load(wv_h, wv)]
    ld_keys = load(keys_h, keys)
    ld_values = load(values_h, values)
    ld_wo = load(wo_h, wo)
    ld_dense += [load(wdg_h, wdg), load(wdu_h, wdu), load(wdd_h, wdd)]
    ld_n2 = [load(ffn_gain_h, ffn_gain), load(mix_h, mixw), load(wr_h, wr)]
    stage("project")
    for copy in ld_tok:
        copy.wait()
    normed = rms_scale(tokens[...], attn_gain[...])
    ld_q.wait()
    queries = dot(normed, wq[...]).astype(BF16)
    for copy in ld_kv:
        copy.wait()
    new_keys[...] = dot_nt(normed, wk[...]).astype(BF16)
    new_values[...] = dot_nt(normed, wv[...]).astype(BF16)
    stores = [
        pltpu.make_async_copy(new_keys, new_keys_h, store_sem.at[0]),
        pltpu.make_async_copy(new_values, new_values_h, store_sem.at[1]),
    ]
    for copy in stores:
        copy.start()

    stage("queries")
    row = iota((128, 1), 0)
    rep = bits(iota((128, ROWS), 0) // 8 == iota((128, ROWS), 1))
    head_lane = iota((128, 512), 1) // 64 == iota((128, 512), 0) % 8
    fold = bits(iota((512, 256), 0) % 64 == iota((512, 256), 1) % 64)
    own_block = iota((128, 256), 1) // 64 == (iota((128, 256), 0) // 8) % 4
    spread = jnp.where(head_lane, dot(rep, queries), 0.0).astype(BF16)
    block_q = jnp.where(own_block, dot(spread, fold), 0.0).astype(BF16)
    bias = jnp.zeros((32, 1), F32)
    for h in range(8):
        bias = jnp.where(iota((32, 1), 0) % 8 == h, head_bias[h], bias)
    after = bits(iota((256, 256), 0) > iota((256, 256), 1))
    stage("cache_wait")
    ld_keys.wait()
    ld_values.wait()
    ld_eg = [load(weg_h, weg), load(weu_h, weu)]
    ld_ed = [load(wed_h.at[:, pl.ds(h * HALF, HALF)], wed.at[h]) for h in range(2)]
    stage("attention")
    mixed = []
    for g in range(4):
        scores = dot(block_q[g * 32 : (g + 1) * 32], keys[pl.ds(g * 256, 256), :]) * 0.125 + bias
        length = jnp.zeros((32, 1), jnp.int32)
        for s in range(4):
            length = jnp.where(iota((32, 1), 0) // 8 == s, lengths[g * 4 + s], length)
        visible = iota((32, 1024), 1) < length
        soft = jnp.log1p(jnp.exp(-jnp.abs(scores)))
        log_take = jnp.minimum(scores, 0.0) - soft
        log_keep = jnp.where(visible, jnp.minimum(-scores, 0.0) - soft, 0.0)
        tiles = jnp.concatenate([log_keep[:, j * 256 : (j + 1) * 256] for j in range(4)], axis=0)
        high, low = two_terms(tiles)
        summed = dot(high, after) + dot(low, after)
        total = summed[:, 0:1] + tiles[:, 0:1]
        later = jnp.zeros((32, 1), F32)
        spans = [None] * 4
        for j in reversed(range(4)):
            spans[j] = summed[j * 32 : (j + 1) * 32] + later
            later = later + total[j * 32 : (j + 1) * 32]
        log_after = jnp.concatenate(spans, axis=1)
        stick = jnp.where(visible, jnp.exp(log_take + log_after), 0.0).astype(BF16)
        mixed.append(dot_nt(stick, values[pl.ds(g * 256, 256), :]))
    mixed = jnp.where(own_block, jnp.concatenate(mixed, axis=0), 0.0).astype(BF16)
    unfold = bits(iota((256, 512), 0) % 64 == iota((256, 512), 1) % 64)
    by_head = jnp.where(head_lane, dot(mixed, unfold), 0.0).astype(BF16)
    gather_rows = bits(iota((ROWS, 128), 1) // 8 == iota((ROWS, 128), 0))
    heads_out = dot(gather_rows, by_head).astype(BF16)
    stage("attention_out")
    ld_dense[0].wait()
    hits_t = jnp.zeros((128, ROWS), F32)
    for k in range(routes.shape[0]):
        hits_t = hits_t + jnp.where(routes[k : k + 1, :] == iota((128, ROWS), 0), 1.0, 0.0)
    eye = bits(iota((ROWS, ROWS), 0) == iota((ROWS, ROWS), 1))
    own_hits = dot_nt(eye, hits_t.astype(BF16))
    hits[0] = own_hits.astype(BF16)
    ld_wo.wait()
    part[...] = dot(heads_out, wo[...]).astype(BF16)
    ap = remote(part, peer_part, ap_s.at[0], ap_r.at[0], partner)
    stage("barrier")
    pl.semaphore_wait(barrier, len(others))
    hz = [remote(hits.at[0], hits.at[d], h_s.at[0], h_r.at[0], at_z(d)) for d in range(1, NZ)]
    ap.start()
    for copy in hz:
        copy.start()
    stage("dense_slices")
    for copy in ld_dense[1:]:
        copy.wait()
    lane = iota((1, NZ * 128), 1)
    first = lax.rem(z + lane // 128, NZ) * 32
    within = lane % 128
    unit = iota((256, NZ * 128), 0)
    pieces = jnp.zeros((ROWS, NZ * 128), F32)
    for k, w in enumerate((wdg[...], wdu[...], wdd[...])):
        target = jnp.where((within >= 32 * k) & (within < 32 * k + 32), first + within - 32 * k, -1)
        pieces = pieces + dot(w, bits(unit == target))
    pieces = pieces.astype(BF16)
    for dz in range(NZ):
        w3p[dz] = pieces[:, dz * 128 : (dz + 1) * 128]
    w3[z, y, x] = w3p[0]

    w3z = [remote(w3p.at[d], w3.at[z, y, x], w3z_s.at[0], w3z_r.at[0], at_z(d)) for d in range(1, NZ)]
    for copy in w3z:
        copy.start()
    first_hop, second_hop = [], []
    for h in range(2):
        zs = pl.ds(4 * h, 4)
        ends = [w3.at[zs, y, x]] * 3, [w3.at[zs, y] if h == 0 else w3.at[zs, :, x]] * 3
        for k, hops in enumerate((first_hop, second_hop)):
            for d in range(1, 4):
                sems = (w3a_s, w3a_r) if k == 0 else (w3b_s, w3b_r)
                to = at_x(d) if h == k else at_y(d)
                hops.append(remote(ends[k][0], ends[k][0], sems[0].at[0], sems[1].at[0], to))


    stage("core_sum")
    for copy in ld_n2:
        copy.wait()
    ap.wait_recv()
    residual = (tokens[...].astype(F32) + (part[...].astype(F32) + peer_part[...].astype(F32))).astype(BF16)
    normed2 = rms_scale(residual, ffn_gain[...])
    for h in range(2):
        resid[h] = residual[:, h * HALF : (h + 1) * HALF]
        for c in range(CHUNKS):
            norm2[h, c] = normed2[:, h * HALF + c * WIDE : h * HALF + (c + 1) * WIDE]
    for c in range(CHUNKS):
        tokf[t, c, 0] = norm2[t, c]
        for d in FAR_Z:
            remote(norm2.at[t, c], tokf.at[t, c, d], tz_s.at[0], tz_r.at[c], at_z(d)).start()
    stage("slots")
    settle(hits.at[pl.ds(1, NZ - 1)], h_r.at[0])
    hit = hits[...].reshape(128, 128)
    base = z * PLANE

    def expert_of(slot):
        d = slot // 16
        return base + lax.rem(y + d // NX, NY) * NX + lax.rem(x + d % NX, NX)

    sel = bits(iota((256, 128), 1) == expert_of(iota((256, 128), 0)))
    tok_r, tok_c = iota((128, 128), 0), iota((128, 128), 1)
    earlier_c = bits((tok_r < tok_c) & (tok_r // 16 == tok_c // 16))
    earlier_r = bits((tok_c < tok_r) & (tok_r // 16 == tok_c // 16))
    slot_hit = dot_nt(sel, hit)
    slot_rank = dot(slot_hit.astype(BF16), earlier_c)
    sr, sc = iota((256, 128), 0), iota((256, 128), 1)
    fits = (slot_rank == ((sr // 8) % 2).astype(F32)) & (sc // 16 == sr % 8)
    dispatch = jnp.where(fits, slot_hit, 0.0).astype(BF16)
    tok_hit = dot_nt(hit, sel)
    tok_rank = dot_nt(dot(earlier_r, hit).astype(BF16), sel)
    cr, cc = iota((128, 256), 0), iota((128, 256), 1)
    taken = (tok_rank == ((cc // 8) % 2).astype(F32)) & (cr // 16 == cc % 8) & (tok_hit > 0.5)

    order = sorted(range(1, PLANE), key=lambda d: -(min(d // NX, NY - d // NX) + min(d % NX, NX - d % NX)))

    def exchange(c, source, target, s_sem, r_sem, where):
        for d in order:
            remote(source.at[c, d], target.at[c, d], s_sem.at[0], r_sem(c, d), where(d)).start()

    def rows_of(ref):
        return ref[...].reshape(-1, WIDE)

    stage("w3z_wait")
    settle(w3p.at[pl.ds(1, NZ - 1)], w3z_r.at[0])
    for copy in first_hop:
        copy.start()
    tf = []
    for c in range(CHUNKS):
        stage("z_gather")
        settle(tokf.at[t, c, pl.ds(1, NZ - 1)], tz_r.at[c])
        stage("dispatch")
        rows = dot(dispatch, rows_of(tokf.at[t, c])).astype(BF16).reshape(PLANE, 16, WIDE)
        for d in range(1, PLANE):
            xs[c, d] = rows[d]
        xin[t, c, 0] = rows[0]
        exchange(c, xs, xin.at[t], xs_s, lambda c, d: xs_r.at[c, d // 4], in_plane)
        tf.append(remote(tokf.at[t, c], tokf.at[t, c], tf_s.at[c], tf_r.at[c], partner))
        tf[c].start()

    stage("plane_hop")
    settle(w3.at[:, pl.ds(0, 3), 0], w3a_r.at[0])
    for copy in second_hop:
        copy.start()
    xf = []
    gate_rows = jnp.zeros((256, 256), F32)
    up_rows = jnp.zeros((256, 256), F32)
    for c in range(CHUNKS):
        stage("plane_in")
        xf.append([])
        for r in range(NY):
            settle(xin.at[t, c, pl.ds(max(1, 4 * r), 3 + (r > 0))], xs_r.at[c, r])
            block = xin.at[t, c, pl.ds(4 * r, 4)]
            xf[c].append(remote(block, block, xf_s.at[0], xf_r.at[c, r], partner))
            xf[c][r].start()
        if c == 0:
            for copy in ld_eg:
                copy.wait()
        stage("expert_own")
        mine, part_w = rows_of(xin.at[t, c]), pl.ds(c * WIDE, WIDE)
        gate_rows = gate_rows + dot(mine, weg[t, part_w])
        up_rows = up_rows + dot(mine, weu[t, part_w])
    for c in range(CHUNKS):
        stage("forward_wait")
        for copy in xf[c]:
            copy.wait_recv()
        stage("expert")
        theirs, part_w = rows_of(xin.at[1 - t, c]), pl.ds(c * WIDE, WIDE)
        gate_rows = gate_rows + dot(theirs, weg[1 - t, part_w])
        up_rows = up_rows + dot(theirs, weu[1 - t, part_w])
    hidden = (gate_rows * sigmoid(gate_rows) * up_rows).astype(BF16)
    for copy in ld_ed:
        copy.wait()
    eo = []
    for c in range(CHUNKS):
        eo_send[c] = dot(hidden, wed[1 - t, :, c * WIDE : (c + 1) * WIDE]).astype(BF16)
        eo.append(remote(eo_send.at[c], eo_peer.at[c], eo_s.at[c], eo_r.at[c], partner))
        eo[c].start()
    for c in range(CHUNKS):
        eo_mine[c] = dot(hidden, wed[t, :, c * WIDE : (c + 1) * WIDE]).astype(BF16)

    for c in range(CHUNKS):
        stage("expert_sum")
        eo[c].wait_recv()
        done = (eo_mine[c].astype(F32) + eo_peer[c].astype(F32)).astype(BF16).reshape(PLANE, 16, WIDE)
        for d in range(1, PLANE):
            ys[c, d] = done[d]
        yr[c, 0] = done[0]
        stage("plane_send")
        exchange(c, ys, yr, ys_s, lambda c, d: ys_r.at[c], back_in_plane)

    stage("dense")
    settle(w3.at[:, pl.ds(0, 3)], w3b_r.at[0])
    pre = jnp.zeros((128, 128), F32)
    zs = WIDE // 256
    for c in range(CHUNKS):
        tf[c].wait_recv()
        for h in range(2):
            pre = pre + dot(rows_of(tokf.at[h, c]), w3[4 * h + zs * c : 4 * h + zs * (c + 1)].reshape(WIDE, 128))
    logits = jnp.zeros((128, 128), F32)
    mix = jnp.zeros((128, 1), F32)
    for c in range(CHUNKS):
        for h in range(2):
            cols = pl.ds(h * HALF + c * WIDE, WIDE)
            block = rows_of(tokf.at[h, c])
            logits = logits + dot(block, wr[cols])
            mix = mix + jnp.sum(block.astype(F32) * mixw[:, cols], axis=-1, keepdims=True)
    mix = sigmoid(mix)
    picked = hit.astype(F32) * sigmoid(logits)
    gates = picked / jnp.sum(picked, axis=-1, keepdims=True) * 2.5
    gate_high, gate_low = two_terms(gates)
    slot_gate = jnp.where(taken, dot_nt(gate_high, sel) + dot_nt(gate_low, sel), 0.0)
    comb_high, comb_low = two_terms(slot_gate)
    gate_in, up_in = pltpu.roll(pre, 64, 1), pltpu.roll(pre, 32, 1)
    used = (iota((128, 128), 1) >= 64) & (iota((128, 128), 1) < 96)
    dense_hidden = jnp.where(used, gate_in * sigmoid(gate_in) * up_in, 0.0).astype(BF16)
    dn_send[...] = dot_nt(dense_hidden, w3[pl.ds(4 * (1 - t), 4)].reshape(HALF, 128)).astype(BF16)
    dn = remote(dn_send, dn_peer, dn_s.at[0], dn_r.at[0], partner)
    dn.start()
    dn_mine[...] = dot_nt(dense_hidden, w3[pl.ds(4 * t, 4)].reshape(HALF, 128)).astype(BF16)

    stage("dense_sum")
    dn.wait_recv()
    dense = mix * (dn_mine[...].astype(F32) + dn_peer[...].astype(F32))
    own = []
    for c in range(CHUNKS):
        stage("plane_back")
        settle(yr.at[c, pl.ds(1, PLANE - 1)], ys_r.at[c])
        stage("combine")
        back = rows_of(yr.at[c])
        sums = dense[:, c * WIDE : (c + 1) * WIDE] + (dot(comb_high, back) + dot(comb_low, back))
        own.append(sums[0:ROWS])
        sums = sums.astype(BF16).reshape(NZ, ROWS, WIDE)
        for d in range(1, NZ):
            ps[c, d] = sums[d]
        for d in FAR_Z:
            remote(ps.at[c, d], pr.at[c, d], ps_s.at[0], ps_r.at[c], at_z(NZ - d)).start()
    for c in range(CHUNKS):
        stage("z_wait")
        settle(pr.at[c, pl.ds(1, NZ - 1)], ps_r.at[c])
        stage("finish")
        total_out = resid[t, :, c * WIDE : (c + 1) * WIDE].astype(F32) + own[c]
        for d in range(1, NZ):
            total_out = total_out + pr[c, d].astype(F32)
        out[c] = total_out.astype(BF16)
        stores.append(
            pltpu.make_async_copy(out.at[c], out_h.at[:, pl.ds(c * WIDE, WIDE)], store_sem.at[2 + c])
        )
        stores[-1].start()
    settle(w3p.at[pl.ds(1, NZ - 1)], w3z_s.at[0])
    settle(hits.at[pl.ds(1, NZ - 1)], h_s.at[0])
    settle(w3.at[:, pl.ds(0, 3), 0], w3a_s.at[0])
    settle(w3.at[:, pl.ds(0, 3)], w3b_s.at[0])
    settle(tokf.at[t, :, pl.ds(1, NZ - 1)], tz_s.at[0])
    settle(xs.at[:, pl.ds(1, PLANE - 1)], xs_s.at[0])
    settle(xin.at[t], xf_s.at[0])
    settle(ys.at[:, pl.ds(1, PLANE - 1)], ys_s.at[0])
    settle(ps.at[:, pl.ds(1, NZ - 1)], ps_s.at[0])
    for copy in [ap, *tf, dn, *eo]:
        copy.wait_send()
    for copy in stores:
        copy.wait()
    stage()


def hand_over(*refs):
    for k in range(3):
        refs[3 + k][...] = refs[k][...]


def shards(
    tokens, lengths, attn_gain, w_query, w_key, w_value, head_bias, key_cache, value_cache, w_attn_out,
    ffn_gain, w_router, routes, w_dense_gate, w_dense_up, w_dense_down, dense_mix,
    w_expert_gate, w_expert_up, w_expert_down,
):
    args = (
        tokens, lengths, attn_gain.reshape(1, WIDTH), w_query, w_key.T, w_value.T, head_bias,
        key_cache.reshape(1024, 1024), value_cache.reshape(1024, 1024), w_attn_out,
        ffn_gain.reshape(1, WIDTH), w_router, routes.T, w_dense_gate, w_dense_up, w_dense_down.T,
        dense_mix.reshape(1, WIDTH), w_expert_gate.reshape(2, HALF, 256), w_expert_up.reshape(2, HALF, 256),
        w_expert_down.reshape(256, WIDTH),
    )
    smem = {1, 6}
    vm, dma = pltpu.VMEM, pltpu.SemaphoreType.DMA
    scratch = [
        vm((CHUNKS, ROWS, WIDE), BF16), vm((ROWS, 64), BF16), vm((ROWS, 64), BF16),
        vm((ROWS, WIDTH), BF16), vm((1, WIDTH), F32), vm((WIDTH, 512), BF16), vm((64, WIDTH), BF16),
        vm((64, WIDTH), BF16), vm((1024, 1024), BF16), vm((1024, 1024), BF16), vm((512, WIDTH), BF16),
        vm((1, WIDTH), F32), vm((WIDTH, 128), BF16), vm((6, ROWS), jnp.int32), vm((ROWS, 256), BF16),
        vm((ROWS, 256), BF16), vm((ROWS, 256), BF16), vm((1, WIDTH), F32),
        vm((2, HALF, 256), BF16), vm((2, HALF, 256), BF16), vm((2, 256, HALF), BF16),
        vm((NZ, ROWS, 128), BF16), vm((NZ, NY, NX, ROWS, 128), BF16), vm((NZ, ROWS, 128), BF16),
        vm((ROWS, WIDTH), BF16), vm((ROWS, WIDTH), BF16),
        vm((2, CHUNKS, ROWS, WIDE), BF16), vm((2, ROWS, HALF), BF16), vm((2, CHUNKS, NZ, ROWS, WIDE), BF16),
        vm((CHUNKS, PLANE, 16, WIDE), BF16), vm((2, CHUNKS, PLANE, 16, WIDE), BF16),
        vm((CHUNKS, 256, WIDE), BF16), vm((CHUNKS, 256, WIDE), BF16), vm((CHUNKS, 256, WIDE), BF16),
        vm((CHUNKS, PLANE, 16, WIDE), BF16), vm((CHUNKS, PLANE, 16, WIDE), BF16),
        vm((128, HALF), BF16), vm((128, HALF), BF16), vm((128, HALF), BF16),
        vm((CHUNKS, NZ, ROWS, WIDE), BF16), vm((CHUNKS, NZ, ROWS, WIDE), BF16),
        dma((LOADS,)), dma((2 + CHUNKS,)),
    ]
    c = CHUNKS
    one, each, quarters = dma((1,)), dma((c,)), dma((c, NY))
    scratch += [one, one] * 5 + [one, each, each, each, one, quarters, one, quarters, each, each, one, each]
    scratch += [one, one, one, each]
    results = pl.pallas_call(
        kernel,
        out_shape=(
            jax.ShapeDtypeStruct((ROWS, HALF), BF16),
            jax.ShapeDtypeStruct((ROWS, 64), BF16),
            jax.ShapeDtypeStruct((ROWS, 64), BF16),
        ),
        in_specs=[
            pl.BlockSpec(memory_space=pltpu.SMEM if k in smem else pl.ANY) for k in range(len(args))
        ],
        out_specs=tuple(pl.BlockSpec(memory_space=pl.ANY) for _ in range(3)),
        scratch_shapes=scratch,
        compiler_params=pltpu.CompilerParams(
            collective_id=0, has_side_effects=True, vmem_limit_bytes=60 * 1024 * 1024
        ),
    )(*args)
    whole = pl.BlockSpec(memory_space=pltpu.VMEM)
    return pl.pallas_call(
        hand_over,
        out_shape=tuple(jax.ShapeDtypeStruct(r.shape, r.dtype) for r in results),
        in_specs=[whole] * 3,
        out_specs=(whole,) * 3,
    )(*results)


def solution(mesh):
    finer = Mesh(mesh.devices.reshape(NZ, NY, NX, mesh.shape["tp"]), ("z", "y", "x", "tp"))
    placed = (
        P(EP, None), P(EP), P(), P(None, "tp"), P(None, "tp"), P(None, "tp"), P("tp"),
        P(EP, "tp", None, None), P(EP, "tp", None, None), P("tp", None), P(), P(), P(EP, None),
        P(EP, "tp"), P(EP, "tp"), P("tp", EP), P(), P(EP, None, "tp"), P(EP, None, "tp"), P(EP, "tp", None),
    )
    return jax.shard_map(
        shards, mesh=finer, in_specs=placed, out_specs=(P(EP, "tp"), P(EP, "tp"), P(EP, "tp")), check_vma=False
    )
```

```python
import jax
import jax.numpy as jnp
from jax import lax
from jax.experimental import pallas as pl
from jax.experimental.pallas import tpu as pltpu
from jax.sharding import Mesh
from jax.sharding import PartitionSpec as P

EP = ("z", "y", "x")
MESH = pl.DeviceIdType.MESH
NZ, NY, NX = 8, 4, 4
PLANE = NY * NX
ROWS, WIDTH, HALF = 16, 2048, 1024
F32, BF16 = jnp.float32, jnp.bfloat16
NT = (((1,), (1,)), ((), ()))
LOADS = 23
CHUNKS = 4
WIDE = HALF // CHUNKS
FAR_Z = (4, 3, 5, 2, 6, 1, 7)


def dot(a, b):
    return jnp.dot(a, b, preferred_element_type=F32)


def dot_nt(a, b):
    return lax.dot_general(a, b, NT, preferred_element_type=F32)


def iota(shape, dim):
    return lax.broadcasted_iota(jnp.int32, shape, dim)


def bits(mask):
    return jnp.where(mask, 1.0, 0.0).astype(BF16)


def two_terms(x):
    high = x.astype(BF16)
    return high, (x - high.astype(F32)).astype(BF16)


def sigmoid(x):
    return 1.0 / (1.0 + jnp.exp(-x))


def rms_scale(values, gain):
    wide = values.astype(F32)
    return (wide * lax.rsqrt(jnp.mean(wide * wide, axis=-1, keepdims=True) + 1e-06) * gain).astype(BF16)


def kernel(
    tokens_h, lengths_h, attn_gain_h, wq_h, wk_h, wv_h, head_bias_h, keys_h, values_h, wo_h,
    ffn_gain_h, wr_h, routes_h, wdg_h, wdu_h, wdd_h, mix_h, weg_h, weu_h, wed_h,
    out, new_keys, new_values,
    tokens, lengths, attn_gain, wq, wk, wv, head_bias, keys, values, wo, ffn_gain, wr, routes, wdg, wdu, wdd, mixw,
    weg, weu, wed,
    w3p, w3, hits, part, peer_part, norm2, resid, tokf, xs, xin, eo_mine, eo_send, eo_peer,
    ys, yr, dn_mine, dn_send, dn_peer, ps, pr,
    load_sem, w3z_s, w3z_r, w3a_s, w3a_r, w3b_s, w3b_r, h_s, h_r, ap_s, ap_r, tz_s, tz_r,
    tf_s, tf_r, xs_s, xs_r, xf_s, xf_r, eo_s, eo_r, ys_s, ys_r, dn_s, dn_r, ps_s, ps_r,
):
    scope = []

    def stage(name=None):
        if scope:
            scope.pop().__exit__(None, None, None)
        if name:
            scope.append(jax.named_scope(name))
            scope[0].__enter__()

    stage("enter")
    z, y, x, t = (lax.axis_index(a) for a in ("z", "y", "x", "tp"))

    def at_z(dz):
        return (lax.rem(z + dz, NZ), y, x, t)

    def at_y(dy):
        return (z, lax.rem(y + dy, NY), x, t)

    def at_x(dx):
        return (z, y, lax.rem(x + dx, NX), t)

    def in_plane(d):
        return (z, lax.rem(y + d // NX, NY), lax.rem(x + d % NX, NX), t)

    def back_in_plane(d):
        return (z, lax.rem(y + NY - d // NX, NY), lax.rem(x + NX - d % NX, NX), t)

    partner = (z, y, x, 1 - t)

    def remote(src, dst, s, r, device):
        return pltpu.make_async_remote_copy(
            src_ref=src, dst_ref=dst, send_sem=s, recv_sem=r, device_id=device, device_id_type=MESH
        )

    def settle(like, sem):
        pltpu.make_async_copy(like, like, sem).wait()

    barrier = pltpu.get_barrier_semaphore()
    others = [at_z(d) for d in range(1, NZ)] + [in_plane(d) for d in range(1, PLANE)] + [partner]
    for device in others:
        pl.semaphore_signal(barrier, inc=1, device_id=device, device_id_type=MESH)

    loads = []

    def load(src, dst):
        copy = pltpu.make_async_copy(src, dst, load_sem.at[len(loads)])
        copy.start()
        loads.append(copy)
        return copy

    ld_tok = [load(tokens_h, tokens), load(attn_gain_h, attn_gain)]
    ld_q = load(wq_h, wq)
    ld_heads = [load(lengths_h, lengths), load(head_bias_h, head_bias)]
    ld_cache = [load(keys_h, keys), load(values_h, values)]
    ld_wo = load(wo_h, wo)
    ld_dense = [load(routes_h, routes), load(wdg_h, wdg), load(wdu_h, wdu), load(wdd_h, wdd)]
    ld_kv = [load(wk_h, wk), load(wv_h, wv)]
    ld_n2 = [load(ffn_gain_h, ffn_gain), load(mix_h, mixw), load(wr_h, wr)]
    stage("project")
    for copy in ld_tok:
        copy.wait()
    normed = rms_scale(tokens[...], attn_gain[...])
    ld_q.wait()
    queries = dot(normed, wq[...]).astype(BF16)
    stage("queries")
    row = iota((128, 1), 0)
    rep = bits(iota((128, ROWS), 0) // 8 == iota((128, ROWS), 1))
    head_lane = iota((128, 512), 1) // 64 == iota((128, 512), 0) % 8
    fold = bits(iota((512, 256), 0) % 64 == iota((512, 256), 1) % 64)
    own_block = iota((128, 256), 1) // 64 == (iota((128, 256), 0) // 8) % 4
    spread = jnp.where(head_lane, dot(rep, queries), 0.0).astype(BF16)
    block_q = jnp.where(own_block, dot(spread, fold), 0.0).astype(BF16)
    for copy in ld_heads:
        copy.wait()
    bias = jnp.zeros((32, 1), F32)
    for h in range(8):
        bias = jnp.where(iota((32, 1), 0) % 8 == h, head_bias[h], bias)
    after = bits(iota((256, 256), 0) > iota((256, 256), 1))
    stage("cache_wait")
    for copy in ld_cache:
        copy.wait()
    stage("attention")
    mixed = []
    for g in range(4):
        scores = dot(block_q[g * 32 : (g + 1) * 32], keys[pl.ds(g * 256, 256), :]) * 0.125 + bias
        length = jnp.zeros((32, 1), jnp.int32)
        for s in range(4):
            length = jnp.where(iota((32, 1), 0) // 8 == s, lengths[g * 4 + s], length)
        visible = iota((32, 1024), 1) < length
        soft = jnp.log1p(jnp.exp(-jnp.abs(scores)))
        log_take = jnp.minimum(scores, 0.0) - soft
        log_keep = jnp.where(visible, jnp.minimum(-scores, 0.0) - soft, 0.0)
        tiles = jnp.concatenate([log_keep[:, j * 256 : (j + 1) * 256] for j in range(4)], axis=0)
        high, low = two_terms(tiles)
        summed = dot(high, after) + dot(low, after)
        total = summed[:, 0:1] + tiles[:, 0:1]
        later = jnp.zeros((32, 1), F32)
        spans = [None] * 4
        for j in reversed(range(4)):
            spans[j] = summed[j * 32 : (j + 1) * 32] + later
            later = later + total[j * 32 : (j + 1) * 32]
        log_after = jnp.concatenate(spans, axis=1)
        stick = jnp.where(visible, jnp.exp(log_take + log_after), 0.0).astype(BF16)
        mixed.append(dot_nt(stick, values[pl.ds(g * 256, 256), :]))
    mixed = jnp.where(own_block, jnp.concatenate(mixed, axis=0), 0.0).astype(BF16)
    unfold = bits(iota((256, 512), 0) % 64 == iota((256, 512), 1) % 64)
    by_head = jnp.where(head_lane, dot(mixed, unfold), 0.0).astype(BF16)
    gather_rows = bits(iota((ROWS, 128), 1) // 8 == iota((ROWS, 128), 0))
    heads_out = dot(gather_rows, by_head).astype(BF16)
    stage("attention_out")
    ld_dense[0].wait()
    hits_t = jnp.zeros((128, ROWS), F32)
    for k in range(routes.shape[0]):
        hits_t = hits_t + jnp.where(routes[k : k + 1, :] == iota((128, ROWS), 0), 1.0, 0.0)
    eye = bits(iota((ROWS, ROWS), 0) == iota((ROWS, ROWS), 1))
    own_hits = dot_nt(eye, hits_t.astype(BF16))
    hits[0] = own_hits.astype(BF16)
    ld_wo.wait()
    ld_eg = [load(weg_h, weg), load(weu_h, weu)]
    ld_ed = [load(wed_h.at[:, pl.ds(h * HALF, HALF)], wed.at[h]) for h in range(2)]
    part[...] = dot(heads_out, wo[...]).astype(BF16)
    ap = remote(part, peer_part, ap_s.at[0], ap_r.at[0], partner)
    stage("barrier")
    pl.semaphore_wait(barrier, len(others))
    hz = [remote(hits.at[0], hits.at[d], h_s.at[0], h_r.at[0], at_z(d)) for d in range(1, NZ)]
    ap.start()
    for copy in hz:
        copy.start()
    stage("dense_slices")
    for copy in ld_dense[1:]:
        copy.wait()
    lane = iota((1, NZ * 128), 1)
    first = lax.rem(z + lane // 128, NZ) * 32
    within = lane % 128
    unit = iota((256, NZ * 128), 0)
    pieces = jnp.zeros((ROWS, NZ * 128), F32)
    for k, w in enumerate((wdg[...], wdu[...], wdd[...])):
        target = jnp.where((within >= 32 * k) & (within < 32 * k + 32), first + within - 32 * k, -1)
        pieces = pieces + dot(w, bits(unit == target))
    pieces = pieces.astype(BF16)
    for dz in range(NZ):
        w3p[dz] = pieces[:, dz * 128 : (dz + 1) * 128]
    w3[z, y, x] = w3p[0]
    for copy in ld_kv:
        copy.wait()
    new_keys[...] = dot_nt(normed, wk[...]).astype(BF16)
    new_values[...] = dot_nt(normed, wv[...]).astype(BF16)


    w3z = [remote(w3p.at[d], w3.at[z, y, x], w3z_s.at[0], w3z_r.at[0], at_z(d)) for d in range(1, NZ)]
    first_hop, second_hop = [], []
    for h in range(2):
        zs = pl.ds(4 * h, 4)
        ends = [w3.at[zs, y, x]] * 3, [w3.at[zs, y] if h == 0 else w3.at[zs, :, x]] * 3
        for k, hops in enumerate((first_hop, second_hop)):
            for d in range(1, 4):
                sems = (w3a_s, w3a_r) if k == 0 else (w3b_s, w3b_r)
                to = at_x(d) if h == k else at_y(d)
                hops.append(remote(ends[k][0], ends[k][0], sems[0].at[0], sems[1].at[0], to))


    stage("core_sum")
    for copy in ld_n2:
        copy.wait()
    ap.wait_recv()
    residual = (tokens[...].astype(F32) + (part[...].astype(F32) + peer_part[...].astype(F32))).astype(BF16)
    normed2 = rms_scale(residual, ffn_gain[...])
    for h in range(2):
        resid[h] = residual[:, h * HALF : (h + 1) * HALF]
        for c in range(CHUNKS):
            norm2[h, c] = normed2[:, h * HALF + c * WIDE : h * HALF + (c + 1) * WIDE]
    for c in range(CHUNKS):
        tokf[t, c, 0] = norm2[t, c]
        for d in FAR_Z:
            remote(norm2.at[t, c], tokf.at[t, c, d], tz_s.at[0], tz_r.at[c], at_z(d)).start()
        if c == 0:
            for copy in w3z:
                copy.start()
    stage("slots")
    settle(hits.at[pl.ds(1, NZ - 1)], h_r.at[0])
    hit = hits[...].reshape(128, 128)
    base = z * PLANE

    def expert_of(slot):
        d = slot // 16
        return base + lax.rem(y + d // NX, NY) * NX + lax.rem(x + d % NX, NX)

    sel = bits(iota((256, 128), 1) == expert_of(iota((256, 128), 0)))
    tok_r, tok_c = iota((128, 128), 0), iota((128, 128), 1)
    earlier_c = bits((tok_r < tok_c) & (tok_r // 16 == tok_c // 16))
    earlier_r = bits((tok_c < tok_r) & (tok_r // 16 == tok_c // 16))
    slot_hit = dot_nt(sel, hit)
    slot_rank = dot(slot_hit.astype(BF16), earlier_c)
    sr, sc = iota((256, 128), 0), iota((256, 128), 1)
    fits = (slot_rank == ((sr // 8) % 2).astype(F32)) & (sc // 16 == sr % 8)
    dispatch = jnp.where(fits, slot_hit, 0.0).astype(BF16)
    tok_hit = dot_nt(hit, sel)
    tok_rank = dot_nt(dot(earlier_r, hit).astype(BF16), sel)
    cr, cc = iota((128, 256), 0), iota((128, 256), 1)
    taken = (tok_rank == ((cc // 8) % 2).astype(F32)) & (cr // 16 == cc % 8) & (tok_hit > 0.5)

    order = sorted(range(1, PLANE), key=lambda d: -(min(d // NX, NY - d // NX) + min(d % NX, NX - d % NX)))

    def exchange(c, source, target, s_sem, r_sem, where):
        for d in order:
            remote(source.at[c, d], target.at[c, d], s_sem.at[0], r_sem(c, d), where(d)).start()

    def rows_of(ref):
        return ref[...].reshape(-1, WIDE)

    tf = []
    for c in range(CHUNKS):
        stage("z_gather")
        settle(tokf.at[t, c, pl.ds(1, NZ - 1)], tz_r.at[c])
        stage("dispatch")
        rows = dot(dispatch, rows_of(tokf.at[t, c])).astype(BF16).reshape(PLANE, 16, WIDE)
        for d in range(1, PLANE):
            xs[c, d] = rows[d]
        xin[t, c, 0] = rows[0]
        exchange(c, xs, xin.at[t], xs_s, lambda c, d: xs_r.at[c, d // 4], in_plane)
        tf.append(remote(tokf.at[t, c], tokf.at[t, c], tf_s.at[c], tf_r.at[c], partner))
        tf[c].start()
        if c == 0:
            stage("w3z_wait")
            settle(w3p.at[pl.ds(1, NZ - 1)], w3z_r.at[0])
            for copy in first_hop:
                copy.start()

    stage("plane_hop")
    settle(w3.at[:, pl.ds(0, 3), 0], w3a_r.at[0])
    for copy in second_hop:
        copy.start()
    xf = []
    gate_rows = jnp.zeros((256, 256), F32)
    up_rows = jnp.zeros((256, 256), F32)
    for c in range(CHUNKS):
        stage("plane_in")
        xf.append([])
        for r in range(NY):
            settle(xin.at[t, c, pl.ds(max(1, 4 * r), 3 + (r > 0))], xs_r.at[c, r])
            block = xin.at[t, c, pl.ds(4 * r, 4)]
            xf[c].append(remote(block, block, xf_s.at[0], xf_r.at[c, r], partner))
            xf[c][r].start()
        if c == 0:
            for copy in ld_eg:
                copy.wait()
        stage("expert_own")
        mine, part_w = rows_of(xin.at[t, c]), pl.ds(c * WIDE, WIDE)
        gate_rows = gate_rows + dot(mine, weg[t, part_w])
        up_rows = up_rows + dot(mine, weu[t, part_w])
    for c in range(CHUNKS):
        stage("forward_wait")
        for copy in xf[c]:
            copy.wait_recv()
        stage("expert")
        theirs, part_w = rows_of(xin.at[1 - t, c]), pl.ds(c * WIDE, WIDE)
        gate_rows = gate_rows + dot(theirs, weg[1 - t, part_w])
        up_rows = up_rows + dot(theirs, weu[1 - t, part_w])
    hidden = (gate_rows * sigmoid(gate_rows) * up_rows).astype(BF16)
    for copy in ld_ed:
        copy.wait()
    eo = []
    for c in range(CHUNKS):
        eo_send[c] = dot(hidden, wed[1 - t, :, c * WIDE : (c + 1) * WIDE]).astype(BF16)
        eo.append(remote(eo_send.at[c], eo_peer.at[c], eo_s.at[c], eo_r.at[c], partner))
        eo[c].start()
    for c in range(CHUNKS):
        eo_mine[c] = dot(hidden, wed[t, :, c * WIDE : (c + 1) * WIDE]).astype(BF16)

    for c in range(CHUNKS):
        stage("expert_sum")
        eo[c].wait_recv()
        done = (eo_mine[c].astype(F32) + eo_peer[c].astype(F32)).astype(BF16).reshape(PLANE, 16, WIDE)
        for d in range(1, PLANE):
            ys[c, d] = done[d]
        yr[c, 0] = done[0]
        stage("plane_send")
        exchange(c, ys, yr, ys_s, lambda c, d: ys_r.at[c], back_in_plane)

    stage("dense")
    settle(w3.at[:, pl.ds(0, 3)], w3b_r.at[0])
    pre = jnp.zeros((128, 128), F32)
    zs = WIDE // 256
    for c in range(CHUNKS):
        tf[c].wait_recv()
        for h in range(2):
            pre = pre + dot(rows_of(tokf.at[h, c]), w3[4 * h + zs * c : 4 * h + zs * (c + 1)].reshape(WIDE, 128))
    logits = jnp.zeros((128, 128), F32)
    mix = jnp.zeros((128, 1), F32)
    for c in range(CHUNKS):
        for h in range(2):
            cols = pl.ds(h * HALF + c * WIDE, WIDE)
            block = rows_of(tokf.at[h, c])
            logits = logits + dot(block, wr[cols])
            mix = mix + jnp.sum(block.astype(F32) * mixw[:, cols], axis=-1, keepdims=True)
    mix = sigmoid(mix)
    picked = hit.astype(F32) * sigmoid(logits)
    gates = picked / jnp.sum(picked, axis=-1, keepdims=True) * 2.5
    gate_high, gate_low = two_terms(gates)
    slot_gate = jnp.where(taken, dot_nt(gate_high, sel) + dot_nt(gate_low, sel), 0.0)
    comb_high, comb_low = two_terms(slot_gate)
    gate_in, up_in = pltpu.roll(pre, 64, 1), pltpu.roll(pre, 32, 1)
    used = (iota((128, 128), 1) >= 64) & (iota((128, 128), 1) < 96)
    dense_hidden = jnp.where(used, gate_in * sigmoid(gate_in) * up_in, 0.0).astype(BF16)
    dn_send[...] = dot_nt(dense_hidden, w3[pl.ds(4 * (1 - t), 4)].reshape(HALF, 128)).astype(BF16)
    dn = remote(dn_send, dn_peer, dn_s.at[0], dn_r.at[0], partner)
    dn.start()
    dn_mine[...] = dot_nt(dense_hidden, w3[pl.ds(4 * t, 4)].reshape(HALF, 128)).astype(BF16)

    stage("dense_sum")
    dn.wait_recv()
    dense = mix * (dn_mine[...].astype(F32) + dn_peer[...].astype(F32))
    own = []
    for c in range(CHUNKS):
        stage("plane_back")
        settle(yr.at[c, pl.ds(1, PLANE - 1)], ys_r.at[c])
        stage("combine")
        back = rows_of(yr.at[c])
        sums = dense[:, c * WIDE : (c + 1) * WIDE] + (dot(comb_high, back) + dot(comb_low, back))
        own.append(sums[0:ROWS])
        sums = sums.astype(BF16).reshape(NZ, ROWS, WIDE)
        for d in range(1, NZ):
            ps[c, d] = sums[d]
        for d in FAR_Z:
            remote(ps.at[c, d], pr.at[c, d], ps_s.at[0], ps_r.at[c], at_z(NZ - d)).start()
    for c in range(CHUNKS):
        stage("z_wait")
        settle(pr.at[c, pl.ds(1, NZ - 1)], ps_r.at[c])
        stage("finish")
        total_out = resid[t, :, c * WIDE : (c + 1) * WIDE].astype(F32) + own[c]
        for d in range(1, NZ):
            total_out = total_out + pr[c, d].astype(F32)
        out[:, c * WIDE : (c + 1) * WIDE] = total_out.astype(BF16)
    settle(w3p.at[pl.ds(1, NZ - 1)], w3z_s.at[0])
    settle(hits.at[pl.ds(1, NZ - 1)], h_s.at[0])
    settle(w3.at[:, pl.ds(0, 3), 0], w3a_s.at[0])
    settle(w3.at[:, pl.ds(0, 3)], w3b_s.at[0])
    settle(tokf.at[t, :, pl.ds(1, NZ - 1)], tz_s.at[0])
    settle(xs.at[:, pl.ds(1, PLANE - 1)], xs_s.at[0])
    settle(xin.at[t], xf_s.at[0])
    settle(ys.at[:, pl.ds(1, PLANE - 1)], ys_s.at[0])
    settle(ps.at[:, pl.ds(1, NZ - 1)], ps_s.at[0])
    for copy in [ap, *tf, dn, *eo]:
        copy.wait_send()
    stage()


def hand_over(*refs):
    for k in range(3):
        refs[3 + k][...] = refs[k][...]


def shards(
    tokens, lengths, attn_gain, w_query, w_key, w_value, head_bias, key_cache, value_cache, w_attn_out,
    ffn_gain, w_router, routes, w_dense_gate, w_dense_up, w_dense_down, dense_mix,
    w_expert_gate, w_expert_up, w_expert_down,
):
    args = (
        tokens, lengths, attn_gain.reshape(1, WIDTH), w_query, w_key.T, w_value.T, head_bias,
        key_cache.reshape(1024, 1024), value_cache.reshape(1024, 1024), w_attn_out,
        ffn_gain.reshape(1, WIDTH), w_router, routes.T, w_dense_gate, w_dense_up, w_dense_down.T,
        dense_mix.reshape(1, WIDTH), w_expert_gate.reshape(2, HALF, 256), w_expert_up.reshape(2, HALF, 256),
        w_expert_down.reshape(256, WIDTH),
    )
    vm, dma = pltpu.VMEM, pltpu.SemaphoreType.DMA
    scratch = [
        vm((ROWS, WIDTH), BF16), pltpu.SMEM((ROWS,), jnp.int32), vm((1, WIDTH), F32), vm((WIDTH, 512), BF16),
        vm((64, WIDTH), BF16), vm((64, WIDTH), BF16), pltpu.SMEM((8,), F32), vm((1024, 1024), BF16), vm((1024, 1024), BF16), vm((512, WIDTH), BF16),
        vm((1, WIDTH), F32), vm((WIDTH, 128), BF16), vm((6, ROWS), jnp.int32), vm((ROWS, 256), BF16),
        vm((ROWS, 256), BF16), vm((ROWS, 256), BF16), vm((1, WIDTH), F32),
        vm((2, HALF, 256), BF16), vm((2, HALF, 256), BF16), vm((2, 256, HALF), BF16),
        vm((NZ, ROWS, 128), BF16), vm((NZ, NY, NX, ROWS, 128), BF16), vm((NZ, ROWS, 128), BF16),
        vm((ROWS, WIDTH), BF16), vm((ROWS, WIDTH), BF16),
        vm((2, CHUNKS, ROWS, WIDE), BF16), vm((2, ROWS, HALF), BF16), vm((2, CHUNKS, NZ, ROWS, WIDE), BF16),
        vm((CHUNKS, PLANE, 16, WIDE), BF16), vm((2, CHUNKS, PLANE, 16, WIDE), BF16),
        vm((CHUNKS, 256, WIDE), BF16), vm((CHUNKS, 256, WIDE), BF16), vm((CHUNKS, 256, WIDE), BF16),
        vm((CHUNKS, PLANE, 16, WIDE), BF16), vm((CHUNKS, PLANE, 16, WIDE), BF16),
        vm((128, HALF), BF16), vm((128, HALF), BF16), vm((128, HALF), BF16),
        vm((CHUNKS, NZ, ROWS, WIDE), BF16), vm((CHUNKS, NZ, ROWS, WIDE), BF16),
        dma((LOADS,)),
    ]
    c = CHUNKS
    one, each, quarters = dma((1,)), dma((c,)), dma((c, NY))
    scratch += [one, one] * 5 + [one, each, each, each, one, quarters, one, quarters, each, each, one, each]
    scratch += [one, one, one, each]
    results = pl.pallas_call(
        kernel,
        out_shape=(
            pltpu.VMEM((ROWS, HALF), BF16),
            pltpu.VMEM((ROWS, 64), BF16),
            pltpu.VMEM((ROWS, 64), BF16),
        ),
        in_specs=[
            pl.BlockSpec(memory_space=pl.ANY) for _ in args
        ],
        out_specs=tuple(pl.BlockSpec(memory_space=pltpu.VMEM) for _ in range(3)),
        scratch_shapes=scratch,
        compiler_params=pltpu.CompilerParams(
            collective_id=0, has_side_effects=True, vmem_limit_bytes=60 * 1024 * 1024
        ),
    )(*args)
    whole = pl.BlockSpec(memory_space=pltpu.VMEM)
    return pl.pallas_call(
        hand_over,
        out_shape=tuple(jax.ShapeDtypeStruct(r.shape, r.dtype) for r in results),
        in_specs=[whole] * 3,
        out_specs=(whole,) * 3,
    )(*(pltpu.with_memory_space_constraint(r, pltpu.VMEM) for r in results))


def solution(mesh):
    finer = Mesh(mesh.devices.reshape(NZ, NY, NX, mesh.shape["tp"]), ("z", "y", "x", "tp"))
    placed = (
        P(EP, None), P(EP), P(), P(None, "tp"), P(None, "tp"), P(None, "tp"), P("tp"),
        P(EP, "tp", None, None), P(EP, "tp", None, None), P("tp", None), P(), P(), P(EP, None),
        P(EP, "tp"), P(EP, "tp"), P("tp", EP), P(), P(EP, None, "tp"), P(EP, None, "tp"), P(EP, "tp", None),
    )
    return jax.shard_map(
        shards, mesh=finer, in_specs=placed, out_specs=(P(EP, "tp"), P(EP, "tp"), P(EP, "tp")), check_vma=False
    )
```

```python
import jax
import jax.numpy as jnp
from jax import lax
from jax.experimental import pallas as pl
from jax.experimental.pallas import tpu as pltpu
from jax.sharding import Mesh
from jax.sharding import PartitionSpec as P

EP = ("z", "y", "x")
MESH = pl.DeviceIdType.MESH
NZ, NY, NX = 8, 4, 4
PLANE = NY * NX
ROWS, WIDTH, HALF = 16, 2048, 1024
F32, BF16 = jnp.float32, jnp.bfloat16
NT = (((1,), (1,)), ((), ()))
LOADS = 23
CHUNKS = 4
WIDE = HALF // CHUNKS
FAR_Z = (4, 3, 5, 2, 6, 1, 7)


def dot(a, b):
    return jnp.dot(a, b, preferred_element_type=F32)


def dot_nt(a, b):
    return lax.dot_general(a, b, NT, preferred_element_type=F32)


def iota(shape, dim):
    return lax.broadcasted_iota(jnp.int32, shape, dim)


def bits(mask):
    return jnp.where(mask, 1.0, 0.0).astype(BF16)


def two_terms(x):
    high = x.astype(BF16)
    return high, (x - high.astype(F32)).astype(BF16)


def sigmoid(x):
    return 1.0 / (1.0 + jnp.exp(-x))


def rms_scale(values, gain):
    wide = values.astype(F32)
    return (wide * lax.rsqrt(jnp.mean(wide * wide, axis=-1, keepdims=True) + 1e-06) * gain).astype(BF16)


def kernel(
    tokens_h, lengths_h, attn_gain_h, wq_h, wk_h, wv_h, head_bias_h, keys_h, values_h, wo_h,
    ffn_gain_h, wr_h, routes_h, wdg_h, wdu_h, wdd_h, mix_h, weg_h, weu_h, wed_h,
    out, new_keys, new_values,
    tokens, lengths, attn_gain, wq, wk, wv, head_bias, keys, values, wo, ffn_gain, wr, routes, wdg, wdu, wdd, mixw,
    weg, weu, wed,
    w3p, w3, hits, part, peer_part, norm2, resid, tokf, xs, xin,
    ys, yr, dn_mine, dn_send, dn_peer, ps, pr,
    load_sem, w3z_s, w3z_r, w3a_s, w3a_r, w3b_s, w3b_r, h_s, h_r, ap_s, ap_r, tz_s, tz_r,
    tf_s, tf_r, xs_s, xs_r, xf_s, xf_r, eo_s, eo_r, ys_s, ys_r, dn_s, dn_r, ps_s, ps_r,
):
    scope = []

    def stage(name=None):
        if scope:
            scope.pop().__exit__(None, None, None)
        if name:
            scope.append(jax.named_scope(name))
            scope[0].__enter__()

    stage("enter")
    z, y, x, t = (lax.axis_index(a) for a in ("z", "y", "x", "tp"))

    def at_z(dz):
        return (lax.rem(z + dz, NZ), y, x, t)

    def at_y(dy):
        return (z, lax.rem(y + dy, NY), x, t)

    def at_x(dx):
        return (z, y, lax.rem(x + dx, NX), t)

    def in_plane(d):
        return (z, lax.rem(y + d // NX, NY), lax.rem(x + d % NX, NX), t)

    def back_in_plane(d):
        return (z, lax.rem(y + NY - d // NX, NY), lax.rem(x + NX - d % NX, NX), t)

    partner = (z, y, x, 1 - t)

    def remote(src, dst, s, r, device):
        return pltpu.make_async_remote_copy(
            src_ref=src, dst_ref=dst, send_sem=s, recv_sem=r, device_id=device, device_id_type=MESH
        )

    def settle(like, sem):
        pltpu.make_async_copy(like, like, sem).wait()

    loads = []

    def load_split(src, dst, pieces):
        sem = load_sem.at[len(loads)]
        rows = src.shape[0] // pieces
        for k in range(pieces):
            pltpu.make_async_copy(src.at[pl.ds(k * rows, rows)], dst.at[pl.ds(k * rows, rows)], sem).start()
        loads.append(pltpu.make_async_copy(src, dst, sem))
        return loads[-1]

    def load(src, dst):
        copy = pltpu.make_async_copy(src, dst, load_sem.at[len(loads)])
        copy.start()
        loads.append(copy)
        return copy

    ld_dense = [load(routes_h, routes), load(wdg_h, wdg), load(wdu_h, wdu), load(wdd_h, wdd)]
    ld_tok = [load(tokens_h, tokens), load(attn_gain_h, attn_gain)]
    ld_q = load(wq_h, wq)
    ld_heads = [load(lengths_h, lengths), load(head_bias_h, head_bias)]
    ld_cache = [load_split(keys_h, keys, 4), load_split(values_h, values, 4)]
    barrier = pltpu.get_barrier_semaphore()
    others = [at_z(d) for d in range(1, NZ)] + [in_plane(d) for d in range(1, PLANE)] + [partner]
    for device in others:
        pl.semaphore_signal(barrier, inc=1, device_id=device, device_id_type=MESH)

    stage("project")
    for copy in ld_tok:
        copy.wait()
    normed = rms_scale(tokens[...], attn_gain[...])
    rep = bits(iota((128, ROWS), 0) // 8 == iota((128, ROWS), 1))
    head_lane = iota((128, 512), 1) // 64 == iota((128, 512), 0) % 8
    fold = bits(iota((512, 256), 0) % 64 == iota((512, 256), 1) % 64)
    own_block = iota((128, 256), 1) // 64 == (iota((128, 256), 0) // 8) % 4
    for copy in ld_heads:
        copy.wait()
    bias = jnp.zeros((32, 1), F32)
    for h in range(8):
        bias = jnp.where(iota((32, 1), 0) % 8 == h, head_bias[h], bias)
    after = bits(iota((256, 256), 0) > iota((256, 256), 1))
    ld_dense[0].wait()
    hits_t = jnp.zeros((128, ROWS), F32)
    for k in range(routes.shape[0]):
        hits_t = hits_t + jnp.where(routes[k : k + 1, :] == iota((128, ROWS), 0), 1.0, 0.0)
    eye = bits(iota((ROWS, ROWS), 0) == iota((ROWS, ROWS), 1))
    own_hits = dot_nt(eye, hits_t.astype(BF16))
    hits[0] = own_hits.astype(BF16)
    for copy in ld_dense[1:]:
        copy.wait()
    lane = iota((1, NZ * 128), 1)
    first = lax.rem(z + lane // 128, NZ) * 32
    within = lane % 128
    unit = iota((256, NZ * 128), 0)
    pieces = jnp.zeros((ROWS, NZ * 128), F32)
    for k, w in enumerate((wdg[...], wdu[...], wdd[...])):
        target = jnp.where((within >= 32 * k) & (within < 32 * k + 32), first + within - 32 * k, -1)
        pieces = pieces + dot(w, bits(unit == target))
    pieces = pieces.astype(BF16)
    for dz in range(NZ):
        w3p[dz] = pieces[:, dz * 128 : (dz + 1) * 128]
    w3[z, y, x] = w3p[0]
    stage("query_wait")
    ld_q.wait()
    ld_wo = load(wo_h, wo)
    ld_kv = [load(wk_h, wk), load(wv_h, wv)]
    ld_n2 = [load(ffn_gain_h, ffn_gain), load(mix_h, mixw), load(wr_h, wr)]
    queries = dot(normed, wq[...]).astype(BF16)
    stage("queries")
    spread = jnp.where(head_lane, dot(rep, queries), 0.0).astype(BF16)
    block_q = jnp.where(own_block, dot(spread, fold), 0.0).astype(BF16)
    stage("cache_wait")
    for copy in ld_cache:
        copy.wait()
    stage("attention")
    mixed = []
    for g in range(4):
        scores = dot(block_q[g * 32 : (g + 1) * 32], keys[pl.ds(g * 256, 256), :]) * 0.125 + bias
        length = jnp.zeros((32, 1), jnp.int32)
        for s in range(4):
            length = jnp.where(iota((32, 1), 0) // 8 == s, lengths[g * 4 + s], length)
        visible = iota((32, 1024), 1) < length
        soft = jnp.log(1.0 + jnp.exp(-jnp.abs(scores)))
        log_take = jnp.minimum(scores, 0.0) - soft
        log_keep = jnp.where(visible, jnp.minimum(-scores, 0.0) - soft, 0.0)
        tiles = jnp.concatenate([log_keep[:, j * 256 : (j + 1) * 256] for j in range(4)], axis=0)
        high, low = two_terms(tiles)
        summed = dot(high, after) + dot(low, after)
        total = summed[:, 0:1] + tiles[:, 0:1]
        later = jnp.zeros((32, 1), F32)
        spans = [None] * 4
        for j in reversed(range(4)):
            spans[j] = summed[j * 32 : (j + 1) * 32] + later
            later = later + total[j * 32 : (j + 1) * 32]
        log_after = jnp.concatenate(spans, axis=1)
        stick = jnp.where(visible, jnp.exp(log_take + log_after), 0.0).astype(BF16)
        mixed.append(dot_nt(stick, values[pl.ds(g * 256, 256), :]))
    mixed = jnp.where(own_block, jnp.concatenate(mixed, axis=0), 0.0).astype(BF16)
    unfold = bits(iota((256, 512), 0) % 64 == iota((256, 512), 1) % 64)
    by_head = jnp.where(head_lane, dot(mixed, unfold), 0.0).astype(BF16)
    gather_rows = bits(iota((ROWS, 128), 1) // 8 == iota((ROWS, 128), 0))
    heads_out = dot(gather_rows, by_head).astype(BF16)
    stage("attention_out")
    ld_wo.wait()
    ld_eg = [load(weg_h, weg.at[0]), load(weu_h, weu.at[0])]
    ld_ed = [load(wed_h.at[:, pl.ds(h * HALF, HALF)], wed.at[0, h]) for h in range(2)]
    part[...] = dot(heads_out, wo[...]).astype(BF16)
    ap = remote(part, peer_part, ap_s.at[0], ap_r.at[0], partner)
    stage("barrier")
    pl.semaphore_wait(barrier, len(others))
    hz = [remote(hits.at[0], hits.at[d], h_s.at[0], h_r.at[0], at_z(d)) for d in range(1, NZ)]
    w3z = [remote(w3p.at[d], w3.at[z, y, x], w3z_s.at[0], w3z_r.at[0], at_z(d)) for d in range(1, NZ)]
    ap.start()
    for copy in hz + w3z:
        copy.start()
    first_hop, second_hop = [], []
    for h in range(2):
        zs = pl.ds(4 * h, 4)
        ends = [w3.at[zs, y, x]] * 3, [w3.at[zs, y] if h == 0 else w3.at[zs, :, x]] * 3
        for k, hops in enumerate((first_hop, second_hop)):
            for d in range(1, 4):
                sems = (w3a_s, w3a_r) if k == 0 else (w3b_s, w3b_r)
                to = at_x(d) if h == k else at_y(d)
                hops.append(remote(ends[k][0], ends[k][0], sems[0].at[0], sems[1].at[0], to))


    stage("core_sum")
    for copy in ld_n2:
        copy.wait()
    ap.wait_recv()
    residual = (tokens[...].astype(F32) + (part[...].astype(F32) + peer_part[...].astype(F32))).astype(BF16)
    normed2 = rms_scale(residual, ffn_gain[...])
    for h in range(2):
        resid[h] = residual[:, h * HALF : (h + 1) * HALF]
        for c in range(CHUNKS):
            norm2[h, c] = normed2[:, h * HALF + c * WIDE : h * HALF + (c + 1) * WIDE]
    for c in range(CHUNKS):
        tokf[t, c, 0] = norm2[t, c]
        for d in FAR_Z:
            remote(norm2.at[t, c], tokf.at[t, c, d], tz_s.at[0], tz_r.at[c], at_z(d)).start()
    stage("new_rows")
    for copy in ld_kv:
        copy.wait()
    new_keys[...] = dot_nt(normed, wk[...]).astype(BF16)
    new_values[...] = dot_nt(normed, wv[...]).astype(BF16)


    stage("weights_send")
    for copy in ld_eg:
        copy.wait()
    shared = [
        remote(weg.at[0], weg.at[1], eo_s.at[0], eo_r.at[0], partner),
        remote(weu.at[0], weu.at[1], eo_s.at[1], eo_r.at[1], partner),
        remote(wed.at[0, 1 - t], wed.at[1, 1 - t], eo_s.at[2], eo_r.at[2], partner),
    ]
    shared[0].start()
    shared[1].start()
    stage("slots")
    settle(hits.at[pl.ds(1, NZ - 1)], h_r.at[0])
    hit = hits[...].reshape(128, 128)
    base = z * PLANE

    def expert_of(slot):
        d = slot // 16
        return base + lax.rem(y + d // NX, NY) * NX + lax.rem(x + d % NX, NX)

    sel = bits(iota((256, 128), 1) == expert_of(iota((256, 128), 0)))
    tok_r, tok_c = iota((128, 128), 0), iota((128, 128), 1)
    earlier_c = bits((tok_r < tok_c) & (tok_r // 16 == tok_c // 16))
    earlier_r = bits((tok_c < tok_r) & (tok_r // 16 == tok_c // 16))
    slot_hit = dot_nt(sel, hit)
    slot_rank = dot(slot_hit.astype(BF16), earlier_c)
    sr, sc = iota((256, 128), 0), iota((256, 128), 1)
    fits = (slot_rank == ((sr // 8) % 2).astype(F32)) & (sc // 16 == sr % 8)
    dispatch = jnp.where(fits, slot_hit, 0.0).astype(BF16)
    tok_hit = dot_nt(hit, sel)
    tok_rank = dot_nt(dot(earlier_r, hit).astype(BF16), sel)
    cr, cc = iota((128, 256), 0), iota((128, 256), 1)
    taken = (tok_rank == ((cc // 8) % 2).astype(F32)) & (cr // 16 == cc % 8) & (tok_hit > 0.5)

    order = sorted(range(1, PLANE), key=lambda d: -(min(d // NX, NY - d // NX) + min(d % NX, NX - d % NX)))

    def exchange(c, source, target, s_sem, r_sem, where):
        for d in order:
            remote(source.at[c, d], target.at[c, d], s_sem.at[0], r_sem(c, d), where(d)).start()

    def rows_of(ref):
        return ref[...].reshape(-1, WIDE)

    tf = []
    for c in range(CHUNKS):
        stage("z_gather")
        settle(tokf.at[t, c, pl.ds(1, NZ - 1)], tz_r.at[c])
        stage("dispatch")
        rows = dot(dispatch, rows_of(tokf.at[t, c])).astype(BF16).reshape(PLANE, 16, WIDE)
        for d in range(1, PLANE):
            xs[c, d] = rows[d]
        xin[t, c, 0] = rows[0]
        exchange(c, xs, xin.at[t], xs_s, lambda c, d: xs_r.at[c, d // 4], in_plane)
        tf.append(remote(tokf.at[t, c], tokf.at[t, c], tf_s.at[c], tf_r.at[c], partner))
        tf[c].start()
        if c == 1:
            for copy in ld_ed:
                copy.wait()
            shared[2].start()
        if c == 0:
            stage("w3z_wait")
            settle(w3p.at[pl.ds(1, NZ - 1)], w3z_r.at[0])
            for copy in first_hop:
                copy.start()

    stage("plane_hop")
    settle(w3.at[:, pl.ds(0, 3), 0], w3a_r.at[0])
    for copy in second_hop:
        copy.start()
    xf = []
    gate_rows = [jnp.zeros((256, 256), F32)] * 2
    up_rows = [jnp.zeros((256, 256), F32)] * 2
    for c in range(CHUNKS):
        stage("plane_in")
        xf.append([])
        for r in range(NY):
            settle(xin.at[t, c, pl.ds(max(1, 4 * r), 3 + (r > 0))], xs_r.at[c, r])
            block = xin.at[t, c, pl.ds(4 * r, 4)]
            xf[c].append(remote(block, block, xf_s.at[0], xf_r.at[c, r], partner))
            xf[c][r].start()
        if c == 0:
            shared[0].wait_recv()
            shared[1].wait_recv()
        stage("expert_own")
        mine, part_w = rows_of(xin.at[t, c]), pl.ds(c * WIDE, WIDE)
        for k in range(2):
            gate_rows[k] = gate_rows[k] + dot(mine, weg[k, t, part_w])
            up_rows[k] = up_rows[k] + dot(mine, weu[k, t, part_w])
    for c in range(CHUNKS):
        stage("forward_wait")
        for copy in xf[c]:
            copy.wait_recv()
        stage("expert")
        theirs, part_w = rows_of(xin.at[1 - t, c]), pl.ds(c * WIDE, WIDE)
        for k in range(2):
            gate_rows[k] = gate_rows[k] + dot(theirs, weg[k, 1 - t, part_w])
            up_rows[k] = up_rows[k] + dot(theirs, weu[k, 1 - t, part_w])
    hidden = [(gate_rows[k] * sigmoid(gate_rows[k]) * up_rows[k]).astype(BF16) for k in range(2)]
    shared[2].wait_recv()
    for c in range(CHUNKS):
        stage("expert_out")
        cols = pl.ds(c * WIDE, WIDE)
        done = dot(hidden[0], wed[0, t, :, cols]) + dot(hidden[1], wed[1, t, :, cols])
        done = done.astype(BF16).reshape(PLANE, 16, WIDE)
        for d in range(1, PLANE):
            ys[c, d] = done[d]
        yr[c, 0] = done[0]
        stage("plane_send")
        exchange(c, ys, yr, ys_s, lambda c, d: ys_r.at[c], back_in_plane)

    stage("dense")
    settle(w3.at[:, pl.ds(0, 3)], w3b_r.at[0])
    pre = jnp.zeros((128, 128), F32)
    zs = WIDE // 256
    for c in range(CHUNKS):
        tf[c].wait_recv()
        for h in range(2):
            pre = pre + dot(rows_of(tokf.at[h, c]), w3[4 * h + zs * c : 4 * h + zs * (c + 1)].reshape(WIDE, 128))
    logits = jnp.zeros((128, 128), F32)
    mix = jnp.zeros((128, 1), F32)
    for c in range(CHUNKS):
        for h in range(2):
            cols = pl.ds(h * HALF + c * WIDE, WIDE)
            block = rows_of(tokf.at[h, c])
            logits = logits + dot(block, wr[cols])
            mix = mix + jnp.sum(block.astype(F32) * mixw[:, cols], axis=-1, keepdims=True)
    mix = sigmoid(mix)
    picked = hit.astype(F32) * sigmoid(logits)
    gates = picked / jnp.sum(picked, axis=-1, keepdims=True) * 2.5
    gate_high, gate_low = two_terms(gates)
    slot_gate = jnp.where(taken, dot_nt(gate_high, sel) + dot_nt(gate_low, sel), 0.0)
    comb_high, comb_low = two_terms(slot_gate)
    gate_in, up_in = pltpu.roll(pre, 64, 1), pltpu.roll(pre, 32, 1)
    used = (iota((128, 128), 1) >= 64) & (iota((128, 128), 1) < 96)
    dense_hidden = jnp.where(used, gate_in * sigmoid(gate_in) * up_in, 0.0).astype(BF16)
    dn_send[...] = dot_nt(dense_hidden, w3[pl.ds(4 * (1 - t), 4)].reshape(HALF, 128)).astype(BF16)
    dn = remote(dn_send, dn_peer, dn_s.at[0], dn_r.at[0], partner)
    dn.start()
    dn_mine[...] = dot_nt(dense_hidden, w3[pl.ds(4 * t, 4)].reshape(HALF, 128)).astype(BF16)

    stage("dense_sum")
    dn.wait_recv()
    dense = mix * (dn_mine[...].astype(F32) + dn_peer[...].astype(F32))
    own = []
    for c in range(CHUNKS):
        stage("plane_back")
        settle(yr.at[c, pl.ds(1, PLANE - 1)], ys_r.at[c])
        stage("combine")
        back = rows_of(yr.at[c])
        sums = dense[:, c * WIDE : (c + 1) * WIDE] + (dot(comb_high, back) + dot(comb_low, back))
        own.append(sums[0:ROWS])
        sums = sums.astype(BF16).reshape(NZ, ROWS, WIDE)
        for d in range(1, NZ):
            ps[c, d] = sums[d]
        for d in FAR_Z:
            remote(ps.at[c, d], pr.at[c, d], ps_s.at[0], ps_r.at[c], at_z(NZ - d)).start()
    for c in range(CHUNKS):
        stage("z_wait")
        settle(pr.at[c, pl.ds(1, NZ - 1)], ps_r.at[c])
        stage("finish")
        total_out = resid[t, :, c * WIDE : (c + 1) * WIDE].astype(F32) + own[c]
        for d in range(1, NZ):
            total_out = total_out + pr[c, d].astype(F32)
        out[:, c * WIDE : (c + 1) * WIDE] = total_out.astype(BF16)
    settle(w3p.at[pl.ds(1, NZ - 1)], w3z_s.at[0])
    settle(hits.at[pl.ds(1, NZ - 1)], h_s.at[0])
    settle(w3.at[:, pl.ds(0, 3), 0], w3a_s.at[0])
    settle(w3.at[:, pl.ds(0, 3)], w3b_s.at[0])
    settle(tokf.at[t, :, pl.ds(1, NZ - 1)], tz_s.at[0])
    settle(xs.at[:, pl.ds(1, PLANE - 1)], xs_s.at[0])
    settle(xin.at[t], xf_s.at[0])
    settle(ys.at[:, pl.ds(1, PLANE - 1)], ys_s.at[0])
    settle(ps.at[:, pl.ds(1, NZ - 1)], ps_s.at[0])
    for copy in [ap, *tf, dn, *shared]:
        copy.wait_send()
    stage()


def hand_over(*refs):
    for k in range(3):
        refs[3 + k][...] = refs[k][...]


def shards(
    tokens, lengths, attn_gain, w_query, w_key, w_value, head_bias, key_cache, value_cache, w_attn_out,
    ffn_gain, w_router, routes, w_dense_gate, w_dense_up, w_dense_down, dense_mix,
    w_expert_gate, w_expert_up, w_expert_down,
):
    args = (
        tokens, lengths, attn_gain.reshape(1, WIDTH), w_query, w_key.T, w_value.T, head_bias,
        key_cache.reshape(1024, 1024), value_cache.reshape(1024, 1024), w_attn_out,
        ffn_gain.reshape(1, WIDTH), w_router, routes.T, w_dense_gate, w_dense_up, w_dense_down.T,
        dense_mix.reshape(1, WIDTH), w_expert_gate.reshape(2, HALF, 256), w_expert_up.reshape(2, HALF, 256),
        w_expert_down.reshape(256, WIDTH),
    )
    vm, dma = pltpu.VMEM, pltpu.SemaphoreType.DMA
    scratch = [
        vm((ROWS, WIDTH), BF16), pltpu.SMEM((ROWS,), jnp.int32), vm((1, WIDTH), F32), vm((WIDTH, 512), BF16),
        vm((64, WIDTH), BF16), vm((64, WIDTH), BF16), pltpu.SMEM((8,), F32), vm((1024, 1024), BF16), vm((1024, 1024), BF16), vm((512, WIDTH), BF16),
        vm((1, WIDTH), F32), vm((WIDTH, 128), BF16), vm((6, ROWS), jnp.int32), vm((ROWS, 256), BF16),
        vm((ROWS, 256), BF16), vm((ROWS, 256), BF16), vm((1, WIDTH), F32),
        vm((2, 2, HALF, 256), BF16), vm((2, 2, HALF, 256), BF16), vm((2, 2, 256, HALF), BF16),
        vm((NZ, ROWS, 128), BF16), vm((NZ, NY, NX, ROWS, 128), BF16), vm((NZ, ROWS, 128), BF16),
        vm((ROWS, WIDTH), BF16), vm((ROWS, WIDTH), BF16),
        vm((2, CHUNKS, ROWS, WIDE), BF16), vm((2, ROWS, HALF), BF16), vm((2, CHUNKS, NZ, ROWS, WIDE), BF16),
        vm((CHUNKS, PLANE, 16, WIDE), BF16), vm((2, CHUNKS, PLANE, 16, WIDE), BF16),
        vm((CHUNKS, PLANE, 16, WIDE), BF16), vm((CHUNKS, PLANE, 16, WIDE), BF16),
        vm((128, HALF), BF16), vm((128, HALF), BF16), vm((128, HALF), BF16),
        vm((CHUNKS, NZ, ROWS, WIDE), BF16), vm((CHUNKS, NZ, ROWS, WIDE), BF16),
        dma((LOADS,)),
    ]
    c = CHUNKS
    one, each, quarters = dma((1,)), dma((c,)), dma((c, NY))
    scratch += [one, one] * 5 + [one, each, each, each, one, quarters, one, quarters, each, each, one, each]
    scratch += [one, one, one, each]
    results = pl.pallas_call(
        kernel,
        out_shape=(
            pltpu.VMEM((ROWS, HALF), BF16),
            pltpu.VMEM((ROWS, 64), BF16),
            pltpu.VMEM((ROWS, 64), BF16),
        ),
        in_specs=[
            pl.BlockSpec(memory_space=pl.ANY) for _ in args
        ],
        out_specs=tuple(pl.BlockSpec(memory_space=pltpu.VMEM) for _ in range(3)),
        scratch_shapes=scratch,
        compiler_params=pltpu.CompilerParams(
            collective_id=0, has_side_effects=True, vmem_limit_bytes=60 * 1024 * 1024
        ),
    )(*args)
    whole = pl.BlockSpec(memory_space=pltpu.VMEM)
    return pl.pallas_call(
        hand_over,
        out_shape=tuple(jax.ShapeDtypeStruct(r.shape, r.dtype) for r in results),
        in_specs=[whole] * 3,
        out_specs=(whole,) * 3,
    )(*(pltpu.with_memory_space_constraint(r, pltpu.VMEM) for r in results))


def solution(mesh):
    finer = Mesh(mesh.devices.reshape(NZ, NY, NX, mesh.shape["tp"]), ("z", "y", "x", "tp"))
    placed = (
        P(EP, None), P(EP), P(), P(None, "tp"), P(None, "tp"), P(None, "tp"), P("tp"),
        P(EP, "tp", None, None), P(EP, "tp", None, None), P("tp", None), P(), P(), P(EP, None),
        P(EP, "tp"), P(EP, "tp"), P("tp", EP), P(), P(EP, None, "tp"), P(EP, None, "tp"), P(EP, "tp", None),
    )
    return jax.shard_map(
        shards, mesh=finer, in_specs=placed, out_specs=(P(EP, "tp"), P(EP, "tp"), P(EP, "tp")), check_vma=False
    )
```

```python
import jax
import jax.numpy as jnp
from jax import lax
from jax.experimental import pallas as pl
from jax.experimental.pallas import tpu as pltpu
from jax.sharding import Mesh
from jax.sharding import PartitionSpec as P

EP = ("z", "y", "x")
MESH = pl.DeviceIdType.MESH
NZ, NY, NX = 8, 4, 4
PLANE = NY * NX
ROWS, WIDTH, HALF = 16, 2048, 1024
F32, BF16 = jnp.float32, jnp.bfloat16
NT = (((1,), (1,)), ((), ()))
LOADS = 23
CHUNKS = 4
WIDE = HALF // CHUNKS
FAR_Z = (4, 3, 5, 2, 6, 1, 7)


def dot(a, b):
    return jnp.dot(a, b, preferred_element_type=F32)


def dot_nt(a, b):
    return lax.dot_general(a, b, NT, preferred_element_type=F32)


def iota(shape, dim):
    return lax.broadcasted_iota(jnp.int32, shape, dim)


def bits(mask):
    return jnp.where(mask, 1.0, 0.0).astype(BF16)


def two_terms(x):
    high = x.astype(BF16)
    return high, (x - high.astype(F32)).astype(BF16)


def sigmoid(x):
    return 1.0 / (1.0 + jnp.exp(-x))


def rms_scale(values, gain):
    wide = values.astype(F32)
    return (wide * lax.rsqrt(jnp.mean(wide * wide, axis=-1, keepdims=True) + 1e-06) * gain).astype(BF16)


def kernel(
    tokens_h, lengths_h, attn_gain_h, wq_h, wk_h, wv_h, head_bias_h, keys_h, values_h, wo_h,
    ffn_gain_h, wr_h, routes_h, wdg_h, wdu_h, wdd_h, mix_h, weg_h, weu_h, wed_h,
    out, new_keys, new_values,
    tokens, lengths, attn_gain, wq, wk, wv, head_bias, keys, values, wo, ffn_gain, wr, routes, wdg, wdu, wdd, mixw,
    weg, weu, wed,
    w3p, w3, hits, part, peer_part, norm2, resid, tokf, xs, xin,
    ys, yr, dn_mine, dn_send, dn_peer, ps, pr,
    load_sem, w3z_s, w3z_r, w3a_s, w3a_r, w3b_s, w3b_r, h_s, h_r, ap_s, ap_r, tz_s, tz_r,
    tf_s, tf_r, xs_s, xs_r, xf_s, xf_r, eo_s, eo_r, ys_s, ys_r, dn_s, dn_r, ps_s, ps_r,
):
    scope = []

    def stage(name=None):
        if scope:
            scope.pop().__exit__(None, None, None)
        if name:
            scope.append(jax.named_scope(name))
            scope[0].__enter__()

    stage("enter")
    z, y, x, t = (lax.axis_index(a) for a in ("z", "y", "x", "tp"))

    def at_z(dz):
        return (lax.rem(z + dz, NZ), y, x, t)

    def at_y(dy):
        return (z, lax.rem(y + dy, NY), x, t)

    def at_x(dx):
        return (z, y, lax.rem(x + dx, NX), t)

    def in_plane(d):
        return (z, lax.rem(y + d // NX, NY), lax.rem(x + d % NX, NX), t)

    def back_in_plane(d):
        return (z, lax.rem(y + NY - d // NX, NY), lax.rem(x + NX - d % NX, NX), t)

    partner = (z, y, x, 1 - t)

    def remote(src, dst, s, r, device):
        return pltpu.make_async_remote_copy(
            src_ref=src, dst_ref=dst, send_sem=s, recv_sem=r, device_id=device, device_id_type=MESH
        )

    def settle(like, sem):
        pltpu.make_async_copy(like, like, sem).wait()

    loads = []

    def load_split(src, dst, pieces):
        sem = load_sem.at[len(loads)]
        rows = src.shape[0] // pieces
        for k in range(pieces):
            pltpu.make_async_copy(src.at[pl.ds(k * rows, rows)], dst.at[pl.ds(k * rows, rows)], sem).start()
        loads.append(pltpu.make_async_copy(src, dst, sem))
        return loads[-1]

    def load(src, dst):
        copy = pltpu.make_async_copy(src, dst, load_sem.at[len(loads)])
        copy.start()
        loads.append(copy)
        return copy

    ld_dense = [load(routes_h, routes), load(wdg_h, wdg), load(wdu_h, wdu), load(wdd_h, wdd)]
    ld_tok = [load(tokens_h, tokens), load(attn_gain_h, attn_gain)]
    ld_q = load(wq_h, wq)
    ld_heads = [load(lengths_h, lengths), load(head_bias_h, head_bias)]
    ld_cache = [load_split(keys_h, keys, 4), load_split(values_h, values, 4)]
    barrier = pltpu.get_barrier_semaphore()
    others = [at_z(d) for d in range(1, NZ)] + [in_plane(d) for d in range(1, PLANE)] + [partner]
    for device in others:
        pl.semaphore_signal(barrier, inc=1, device_id=device, device_id_type=MESH)

    stage("project")
    for copy in ld_tok:
        copy.wait()
    normed = rms_scale(tokens[...], attn_gain[...])
    rep = bits(iota((128, ROWS), 0) // 8 == iota((128, ROWS), 1))
    head_lane = iota((128, 512), 1) // 64 == iota((128, 512), 0) % 8
    fold = bits(iota((512, 256), 0) % 64 == iota((512, 256), 1) % 64)
    own_block = iota((128, 256), 1) // 64 == (iota((128, 256), 0) // 8) % 4
    for copy in ld_heads:
        copy.wait()
    bias = jnp.zeros((32, 1), F32)
    for h in range(8):
        bias = jnp.where(iota((32, 1), 0) % 8 == h, head_bias[h], bias)
    after = bits(iota((256, 256), 0) > iota((256, 256), 1))
    ld_dense[0].wait()
    hits_t = jnp.zeros((128, ROWS), F32)
    for k in range(routes.shape[0]):
        hits_t = hits_t + jnp.where(routes[k : k + 1, :] == iota((128, ROWS), 0), 1.0, 0.0)
    eye = bits(iota((ROWS, ROWS), 0) == iota((ROWS, ROWS), 1))
    own_hits = dot_nt(eye, hits_t.astype(BF16))
    hits[0] = own_hits.astype(BF16)
    for copy in ld_dense[1:]:
        copy.wait()
    lane = iota((1, NZ * 128), 1)
    first = lax.rem(z + lane // 128, NZ) * 32
    within = lane % 128
    unit = iota((256, NZ * 128), 0)
    pieces = jnp.zeros((ROWS, NZ * 128), F32)
    for k, w in enumerate((wdg[...], wdu[...], wdd[...])):
        target = jnp.where((within >= 32 * k) & (within < 32 * k + 32), first + within - 32 * k, -1)
        pieces = pieces + dot(w, bits(unit == target))
    pieces = pieces.astype(BF16)
    for dz in range(NZ):
        w3p[dz] = pieces[:, dz * 128 : (dz + 1) * 128]
    w3[z, y, x] = w3p[0]
    stage("query_wait")
    ld_q.wait()
    ld_wo = load(wo_h, wo)
    ld_kv = [load(wk_h, wk), load(wv_h, wv)]
    ld_n2 = [load(ffn_gain_h, ffn_gain), load(mix_h, mixw), load(wr_h, wr)]
    queries = dot(normed, wq[...]).astype(BF16)
    stage("queries")
    spread = jnp.where(head_lane, dot(rep, queries), 0.0).astype(BF16)
    block_q = jnp.where(own_block, dot(spread, fold), 0.0).astype(BF16)
    stage("cache_wait")
    for copy in ld_cache:
        copy.wait()
    stage("attention")
    mixed = []
    for g in range(4):
        scores = dot(block_q[g * 32 : (g + 1) * 32], keys[pl.ds(g * 256, 256), :]) * 0.125 + bias
        length = jnp.zeros((32, 1), jnp.int32)
        for s in range(4):
            length = jnp.where(iota((32, 1), 0) // 8 == s, lengths[g * 4 + s], length)
        visible = iota((32, 1024), 1) < length
        soft = jnp.log(1.0 + jnp.exp(-jnp.abs(scores)))
        log_take = jnp.minimum(scores, 0.0) - soft
        log_keep = jnp.where(visible, jnp.minimum(-scores, 0.0) - soft, 0.0)
        tiles = jnp.concatenate([log_keep[:, j * 256 : (j + 1) * 256] for j in range(4)], axis=0)
        high, low = two_terms(tiles)
        summed = dot(high, after) + dot(low, after)
        total = summed[:, 0:1] + tiles[:, 0:1]
        later = jnp.zeros((32, 1), F32)
        spans = [None] * 4
        for j in reversed(range(4)):
            spans[j] = summed[j * 32 : (j + 1) * 32] + later
            later = later + total[j * 32 : (j + 1) * 32]
        log_after = jnp.concatenate(spans, axis=1)
        stick = jnp.where(visible, jnp.exp(log_take + log_after), 0.0).astype(BF16)
        mixed.append(dot_nt(stick, values[pl.ds(g * 256, 256), :]))
    mixed = jnp.where(own_block, jnp.concatenate(mixed, axis=0), 0.0).astype(BF16)
    unfold = bits(iota((256, 512), 0) % 64 == iota((256, 512), 1) % 64)
    by_head = jnp.where(head_lane, dot(mixed, unfold), 0.0).astype(BF16)
    gather_rows = bits(iota((ROWS, 128), 1) // 8 == iota((ROWS, 128), 0))
    heads_out = dot(gather_rows, by_head).astype(BF16)
    stage("attention_out")
    ld_wo.wait()
    ld_eg = [load(weg_h, weg.at[0]), load(weu_h, weu.at[0])]
    ld_ed = [load(wed_h.at[:, pl.ds(h * HALF, HALF)], wed.at[0, h]) for h in range(2)]
    part[...] = dot(heads_out, wo[...]).astype(BF16)
    ap = remote(part, peer_part, ap_s.at[0], ap_r.at[0], partner)
    stage("barrier")
    pl.semaphore_wait(barrier, len(others))
    hz = [remote(hits.at[0], hits.at[d], h_s.at[0], h_r.at[0], at_z(d)) for d in range(1, NZ)]
    w3z = [remote(w3p.at[d], w3.at[z, y, x], w3z_s.at[0], w3z_r.at[0], at_z(d)) for d in range(1, NZ)]
    ap.start()
    for copy in hz + w3z:
        copy.start()
    first_hop, second_hop = [], []
    for h in range(2):
        zs = pl.ds(4 * h, 4)
        ends = [w3.at[zs, y, x]] * 3, [w3.at[zs, y] if h == 0 else w3.at[zs, :, x]] * 3
        for k, hops in enumerate((first_hop, second_hop)):
            for d in range(1, 4):
                sems = (w3a_s, w3a_r) if k == 0 else (w3b_s, w3b_r)
                to = at_x(d) if h == k else at_y(d)
                hops.append(remote(ends[k][0], ends[k][0], sems[0].at[0], sems[1].at[0], to))


    stage("core_sum")
    for copy in ld_n2:
        copy.wait()
    ap.wait_recv()
    residual = (tokens[...].astype(F32) + (part[...].astype(F32) + peer_part[...].astype(F32))).astype(BF16)
    normed2 = rms_scale(residual, ffn_gain[...])
    for h in range(2):
        resid[h] = residual[:, h * HALF : (h + 1) * HALF]
        for c in range(CHUNKS):
            norm2[h, c] = normed2[:, h * HALF + c * WIDE : h * HALF + (c + 1) * WIDE]
    for c in range(CHUNKS):
        tokf[t, c, 0] = norm2[t, c]
        for d in FAR_Z:
            remote(norm2.at[t, c], tokf.at[t, c, d], tz_s.at[0], tz_r.at[c], at_z(d)).start()
    stage("new_rows")
    for copy in ld_kv:
        copy.wait()
    new_keys[...] = dot_nt(normed, wk[...]).astype(BF16)
    new_values[...] = dot_nt(normed, wv[...]).astype(BF16)


    stage("weights_send")
    for copy in ld_eg:
        copy.wait()
    shared = [
        remote(weg.at[0], weg.at[1], eo_s.at[0], eo_r.at[0], partner),
        remote(weu.at[0], weu.at[1], eo_s.at[1], eo_r.at[1], partner),
        remote(wed.at[0, 1 - t], wed.at[1, 1 - t], eo_s.at[2], eo_r.at[2], partner),
    ]
    shared[0].start()
    shared[1].start()
    stage("slots")
    settle(hits.at[pl.ds(1, NZ - 1)], h_r.at[0])
    hit = hits[...].reshape(128, 128)
    base = z * PLANE

    def expert_of(slot):
        d = slot // 16
        return base + lax.rem(y + d // NX, NY) * NX + lax.rem(x + d % NX, NX)

    sel = bits(iota((256, 128), 1) == expert_of(iota((256, 128), 0)))
    tok_r, tok_c = iota((128, 128), 0), iota((128, 128), 1)
    earlier_c = bits((tok_r < tok_c) & (tok_r // 16 == tok_c // 16))
    earlier_r = bits((tok_c < tok_r) & (tok_r // 16 == tok_c // 16))
    slot_hit = dot_nt(sel, hit)
    slot_rank = dot(slot_hit.astype(BF16), earlier_c)
    sr, sc = iota((256, 128), 0), iota((256, 128), 1)
    fits = (slot_rank == ((sr // 8) % 2).astype(F32)) & (sc // 16 == sr % 8)
    dispatch = jnp.where(fits, slot_hit, 0.0).astype(BF16)
    tok_hit = dot_nt(hit, sel)
    tok_rank = dot_nt(dot(earlier_r, hit).astype(BF16), sel)
    cr, cc = iota((128, 256), 0), iota((128, 256), 1)
    taken = (tok_rank == ((cc // 8) % 2).astype(F32)) & (cr // 16 == cc % 8) & (tok_hit > 0.5)

    order = sorted(range(1, PLANE), key=lambda d: -(min(d // NX, NY - d // NX) + min(d % NX, NX - d % NX)))

    def exchange(c, source, target, s_sem, r_sem, where):
        for d in order:
            remote(source.at[c, d], target.at[c, d], s_sem.at[0], r_sem(c, d), where(d)).start()

    def rows_of(ref):
        return ref[...].reshape(-1, WIDE)

    tf = []
    for c in range(CHUNKS):
        stage("z_gather")
        settle(tokf.at[t, c, pl.ds(1, NZ - 1)], tz_r.at[c])
        stage("dispatch")
        rows = dot(dispatch, rows_of(tokf.at[t, c])).astype(BF16).reshape(PLANE, 16, WIDE)
        for d in range(1, PLANE):
            xs[c, d] = rows[d]
        xin[t, c, 0] = rows[0]
        exchange(c, xs, xin.at[t], xs_s, lambda c, d: xs_r.at[c, d // 4], in_plane)
        tf.append(remote(tokf.at[t, c], tokf.at[t, c], tf_s.at[c], tf_r.at[c], partner))
        tf[c].start()
        if c == 1:
            for copy in ld_ed:
                copy.wait()
            shared[2].start()
        if c == 0:
            stage("w3z_wait")
            settle(w3p.at[pl.ds(1, NZ - 1)], w3z_r.at[0])
            for copy in first_hop:
                copy.start()

    xf = []
    gate_rows = [jnp.zeros((256, 256), F32)] * 2
    up_rows = [jnp.zeros((256, 256), F32)] * 2
    for c in range(CHUNKS):
        stage("plane_in")
        xf.append([])
        for r in range(NY):
            settle(xin.at[t, c, pl.ds(max(1, 4 * r), 3 + (r > 0))], xs_r.at[c, r])
            block = xin.at[t, c, pl.ds(4 * r, 4)]
            xf[c].append(remote(block, block, xf_s.at[0], xf_r.at[c, r], partner))
            xf[c][r].start()
        if c == 0:
            shared[0].wait_recv()
            shared[1].wait_recv()
        if c == 1:
            stage("plane_hop")
            settle(w3.at[:, pl.ds(0, 3), 0], w3a_r.at[0])
            for copy in second_hop:
                copy.start()
        stage("expert_own")
        mine, part_w = rows_of(xin.at[t, c]), pl.ds(c * WIDE, WIDE)
        for k in range(2):
            gate_rows[k] = gate_rows[k] + dot(mine, weg[k, t, part_w])
            up_rows[k] = up_rows[k] + dot(mine, weu[k, t, part_w])
    for c in range(CHUNKS):
        stage("forward_wait")
        for copy in xf[c]:
            copy.wait_recv()
        stage("expert")
        theirs, part_w = rows_of(xin.at[1 - t, c]), pl.ds(c * WIDE, WIDE)
        for k in range(2):
            gate_rows[k] = gate_rows[k] + dot(theirs, weg[k, 1 - t, part_w])
            up_rows[k] = up_rows[k] + dot(theirs, weu[k, 1 - t, part_w])
    hidden = [(gate_rows[k] * sigmoid(gate_rows[k]) * up_rows[k]).astype(BF16) for k in range(2)]
    shared[2].wait_recv()
    for c in range(CHUNKS):
        stage("expert_out")
        cols = pl.ds(c * WIDE, WIDE)
        done = dot(hidden[0], wed[0, t, :, cols]) + dot(hidden[1], wed[1, t, :, cols])
        done = done.astype(BF16).reshape(PLANE, 16, WIDE)
        for d in range(1, PLANE):
            ys[c, d] = done[d]
        yr[c, 0] = done[0]
        stage("plane_send")
        exchange(c, ys, yr, ys_s, lambda c, d: ys_r.at[c], back_in_plane)

    stage("dense")
    settle(w3.at[:, pl.ds(0, 3)], w3b_r.at[0])
    pre = jnp.zeros((128, 128), F32)
    zs = WIDE // 256
    for c in range(CHUNKS):
        tf[c].wait_recv()
        for h in range(2):
            pre = pre + dot(rows_of(tokf.at[h, c]), w3[4 * h + zs * c : 4 * h + zs * (c + 1)].reshape(WIDE, 128))
    logits = jnp.zeros((128, 128), F32)
    mix = jnp.zeros((128, 1), F32)
    for c in range(CHUNKS):
        for h in range(2):
            cols = pl.ds(h * HALF + c * WIDE, WIDE)
            block = rows_of(tokf.at[h, c])
            logits = logits + dot(block, wr[cols])
            mix = mix + jnp.sum(block.astype(F32) * mixw[:, cols], axis=-1, keepdims=True)
    mix = sigmoid(mix)
    picked = hit.astype(F32) * sigmoid(logits)
    gates = picked / jnp.sum(picked, axis=-1, keepdims=True) * 2.5
    gate_high, gate_low = two_terms(gates)
    slot_gate = jnp.where(taken, dot_nt(gate_high, sel) + dot_nt(gate_low, sel), 0.0)
    comb_high, comb_low = two_terms(slot_gate)
    gate_in, up_in = pltpu.roll(pre, 64, 1), pltpu.roll(pre, 32, 1)
    used = (iota((128, 128), 1) >= 64) & (iota((128, 128), 1) < 96)
    dense_hidden = jnp.where(used, gate_in * sigmoid(gate_in) * up_in, 0.0).astype(BF16)
    dn_send[...] = dot_nt(dense_hidden, w3[pl.ds(4 * (1 - t), 4)].reshape(HALF, 128)).astype(BF16)
    dn = remote(dn_send, dn_peer, dn_s.at[0], dn_r.at[0], partner)
    dn.start()
    dn_mine[...] = dot_nt(dense_hidden, w3[pl.ds(4 * t, 4)].reshape(HALF, 128)).astype(BF16)

    stage("dense_sum")
    dn.wait_recv()
    dense = mix * (dn_mine[...].astype(F32) + dn_peer[...].astype(F32))
    own = []
    for c in range(CHUNKS):
        stage("plane_back")
        settle(yr.at[c, pl.ds(1, PLANE - 1)], ys_r.at[c])
        stage("combine")
        back = rows_of(yr.at[c])
        sums = dense[:, c * WIDE : (c + 1) * WIDE] + (dot(comb_high, back) + dot(comb_low, back))
        own.append(sums[0:ROWS])
        sums = sums.astype(BF16).reshape(NZ, ROWS, WIDE)
        for d in range(1, NZ):
            ps[c, d] = sums[d]
        for d in FAR_Z:
            remote(ps.at[c, d], pr.at[c, d], ps_s.at[0], ps_r.at[c], at_z(NZ - d)).start()
    for c in range(CHUNKS):
        stage("z_wait")
        settle(pr.at[c, pl.ds(1, NZ - 1)], ps_r.at[c])
        stage("finish")
        total_out = resid[t, :, c * WIDE : (c + 1) * WIDE].astype(F32) + own[c]
        for d in range(1, NZ):
            total_out = total_out + pr[c, d].astype(F32)
        out[:, c * WIDE : (c + 1) * WIDE] = total_out.astype(BF16)
    settle(w3p.at[pl.ds(1, NZ - 1)], w3z_s.at[0])
    settle(hits.at[pl.ds(1, NZ - 1)], h_s.at[0])
    settle(w3.at[:, pl.ds(0, 3), 0], w3a_s.at[0])
    settle(w3.at[:, pl.ds(0, 3)], w3b_s.at[0])
    settle(tokf.at[t, :, pl.ds(1, NZ - 1)], tz_s.at[0])
    settle(xs.at[:, pl.ds(1, PLANE - 1)], xs_s.at[0])
    settle(xin.at[t], xf_s.at[0])
    settle(ys.at[:, pl.ds(1, PLANE - 1)], ys_s.at[0])
    settle(ps.at[:, pl.ds(1, NZ - 1)], ps_s.at[0])
    for copy in [ap, *tf, dn, *shared]:
        copy.wait_send()
    stage()


def hand_over(*refs):
    for k in range(3):
        refs[3 + k][...] = refs[k][...]


def shards(
    tokens, lengths, attn_gain, w_query, w_key, w_value, head_bias, key_cache, value_cache, w_attn_out,
    ffn_gain, w_router, routes, w_dense_gate, w_dense_up, w_dense_down, dense_mix,
    w_expert_gate, w_expert_up, w_expert_down,
):
    args = (
        tokens, lengths, attn_gain.reshape(1, WIDTH), w_query, w_key.T, w_value.T, head_bias,
        key_cache.reshape(1024, 1024), value_cache.reshape(1024, 1024), w_attn_out,
        ffn_gain.reshape(1, WIDTH), w_router, routes.T, w_dense_gate, w_dense_up, w_dense_down.T,
        dense_mix.reshape(1, WIDTH), w_expert_gate.reshape(2, HALF, 256), w_expert_up.reshape(2, HALF, 256),
        w_expert_down.reshape(256, WIDTH),
    )
    vm, dma = pltpu.VMEM, pltpu.SemaphoreType.DMA
    scratch = [
        vm((ROWS, WIDTH), BF16), pltpu.SMEM((ROWS,), jnp.int32), vm((1, WIDTH), F32), vm((WIDTH, 512), BF16),
        vm((64, WIDTH), BF16), vm((64, WIDTH), BF16), pltpu.SMEM((8,), F32), vm((1024, 1024), BF16), vm((1024, 1024), BF16), vm((512, WIDTH), BF16),
        vm((1, WIDTH), F32), vm((WIDTH, 128), BF16), vm((6, ROWS), jnp.int32), vm((ROWS, 256), BF16),
        vm((ROWS, 256), BF16), vm((ROWS, 256), BF16), vm((1, WIDTH), F32),
        vm((2, 2, HALF, 256), BF16), vm((2, 2, HALF, 256), BF16), vm((2, 2, 256, HALF), BF16),
        vm((NZ, ROWS, 128), BF16), vm((NZ, NY, NX, ROWS, 128), BF16), vm((NZ, ROWS, 128), BF16),
        vm((ROWS, WIDTH), BF16), vm((ROWS, WIDTH), BF16),
        vm((2, CHUNKS, ROWS, WIDE), BF16), vm((2, ROWS, HALF), BF16), vm((2, CHUNKS, NZ, ROWS, WIDE), BF16),
        vm((CHUNKS, PLANE, 16, WIDE), BF16), vm((2, CHUNKS, PLANE, 16, WIDE), BF16),
        vm((CHUNKS, PLANE, 16, WIDE), BF16), vm((CHUNKS, PLANE, 16, WIDE), BF16),
        vm((128, HALF), BF16), vm((128, HALF), BF16), vm((128, HALF), BF16),
        vm((CHUNKS, NZ, ROWS, WIDE), BF16), vm((CHUNKS, NZ, ROWS, WIDE), BF16),
        dma((LOADS,)),
    ]
    c = CHUNKS
    one, each, quarters = dma((1,)), dma((c,)), dma((c, NY))
    scratch += [one, one] * 5 + [one, each, each, each, one, quarters, one, quarters, each, each, one, each]
    scratch += [one, one, one, each]
    results = pl.pallas_call(
        kernel,
        out_shape=(
            pltpu.VMEM((ROWS, HALF), BF16),
            pltpu.VMEM((ROWS, 64), BF16),
            pltpu.VMEM((ROWS, 64), BF16),
        ),
        in_specs=[
            pl.BlockSpec(memory_space=pl.ANY) for _ in args
        ],
        out_specs=tuple(pl.BlockSpec(memory_space=pltpu.VMEM) for _ in range(3)),
        scratch_shapes=scratch,
        compiler_params=pltpu.CompilerParams(
            collective_id=0, has_side_effects=True, vmem_limit_bytes=60 * 1024 * 1024
        ),
    )(*args)
    whole = pl.BlockSpec(memory_space=pltpu.VMEM)
    return pl.pallas_call(
        hand_over,
        out_shape=tuple(jax.ShapeDtypeStruct(r.shape, r.dtype) for r in results),
        in_specs=[whole] * 3,
        out_specs=(whole,) * 3,
    )(*(pltpu.with_memory_space_constraint(r, pltpu.VMEM) for r in results))


def solution(mesh):
    finer = Mesh(mesh.devices.reshape(NZ, NY, NX, mesh.shape["tp"]), ("z", "y", "x", "tp"))
    placed = (
        P(EP, None), P(EP), P(), P(None, "tp"), P(None, "tp"), P(None, "tp"), P("tp"),
        P(EP, "tp", None, None), P(EP, "tp", None, None), P("tp", None), P(), P(), P(EP, None),
        P(EP, "tp"), P(EP, "tp"), P("tp", EP), P(), P(EP, None, "tp"), P(EP, None, "tp"), P(EP, "tp", None),
    )
    return jax.shard_map(
        shards, mesh=finer, in_specs=placed, out_specs=(P(EP, "tp"), P(EP, "tp"), P(EP, "tp")), check_vma=False
    )
```
